512 devices in a mesh: sp: 64 (over z, y), tp: 8 (over x, core).
Axes of the slice: x: 4, y: 8, z: 8, core: 2. Of those that a mesh axis runs over, the one named last changes fastest.
Arguments:
- resid: bfloat16 [12288, 2048], P(('sp', 'tp')), may hold values from -6 to 6
- queries: bfloat16 [12288, 2048], P('sp', 'tp'), may hold values from -8 to 8
- keys: bfloat16 [12288, 512], P('sp', 'tp'), may hold values from -8 to 8
- values: bfloat16 [12288, 512], P('sp', 'tp'), may hold values from -6 to 6
- log_gates: float32 [12288, 32], P('sp', 'tp'), may hold values from -6144 to 0, as said below
- out_gate: bfloat16 [12288, 2048], P('sp', 'tp'), may hold values from -8 to 8
- out_weight: bfloat16 [2048, 2048], P('tp'), may hold values from -0.125 to 0.125
- post_gain: float32 [2048], replicated, may hold values from 0.1 to 1.9
- pre_gain: float32 [2048], replicated, may hold values from 0.1 to 1.9
- ffn_gain: float32 [2048], replicated, may hold values from 0.1 to 1.9
- gate_weight: bfloat16 [2048, 5632], P('sp', 'tp'), may hold values from -0.125 to 0.125
- up_weight: bfloat16 [2048, 5632], P('sp', 'tp'), may hold values from -0.125 to 0.125
- down_weight: bfloat16 [5632, 2048], P('tp', 'sp'), may hold values from -0.078125 to 0.078125
Outputs:
- result: bfloat16 [12288, 2048], P(('sp', 'tp'))
The draws below stay inside these ranges and needn't reach their ends.
Inputs may be any that keep to these rules, and one draw needn't show every extreme that they name: Each head's column of log_gates never rises from one position to the next, and its first entry is at most 0.
All inputs are finite; a program needn't handle non-finite values.
Results may differ from the reference program's by a relative error of at most 0.017.
Values may be sent and summed in bfloat16 or wider, within the bound.
No kernel may reach another device: no remote copies, remote signals or barrier semaphores. Data moves between devices by JAX's collectives and lax.ppermute only.
A program may use at most 64 MiB of HBM per device.

```python
import math
import jax
import jax.numpy as jnp
from jax import lax

D = 2048
H = 32
KV = 8
HD = 64
FF = 5632
TOK_DEV = 192
TOKENS = 12288


def base_field(key, shape):
    return jnp.clip(jax.random.normal(key, shape, jnp.float32), -4.0, 4.0)


def draw_queries(key, part):
    field = base_field(jax.random.fold_in(key, 11), (TOKENS, H * HD))
    return field.astype(jnp.bfloat16)


def draw_keys(key, part):
    field = base_field(jax.random.fold_in(key, 13), (TOKENS, KV * HD))
    return field.astype(jnp.bfloat16)


def draw_log_gates(key, part):
    keyring = jax.random.split(jax.random.fold_in(key, 17), 5)
    order = jax.random.permutation(keyring[0], H)
    slow = order >= H // 2
    rate = jnp.where(slow, 0.5 / TOKENS, 1.0 / 40.0).astype(jnp.float32)
    blocks = TOKENS // TOK_DEV
    block_factor = jnp.exp(jax.random.uniform(keyring[1], (blocks,), jnp.float32, math.log(0.4), math.log(2.5)))
    block_factor = jnp.repeat(block_factor, TOK_DEV)[:, None]
    data = jnp.exp(0.6 * jnp.clip(jax.random.normal(keyring[2], (TOKENS, H), jnp.float32), -3.0, 3.0))
    steps = -rate[None, :] * block_factor * data
    hits = jax.random.uniform(keyring[3], (TOKENS, H), jnp.float32) < 2.0 / TOKENS
    loss = jax.random.uniform(keyring[4], (TOKENS, H), jnp.float32, 0.2, 0.5)
    steps = steps + jnp.where(hits & slow[None, :], jnp.log(1.0 - loss), 0.0)
    return jnp.cumsum(steps, axis=0).astype(jnp.float32)


def block_scale(rng, extent, cuts, least, top_value):
    def one(dim, shards_of):
        draws = jax.random.uniform(jax.random.fold_in(jax.random.fold_in(rng, 6), dim), (shards_of,), jnp.float32, least / len(cuts), top_value / len(cuts))
        return jnp.repeat(jnp.exp(draws), extent[dim] // shards_of).reshape((-1,) + (1,) * (len(extent) - dim - 1))

    level = one(*cuts[0])
    for cut in cuts[1:]:
        level = level * one(*cut)
    return level


def centred(own_key, extent, deviation, reach, cuts=(), kind=jnp.bfloat16):
    level = block_scale(own_key, extent, cuts, -0.22, 0.18) if cuts else 1.0
    entries = jax.random.normal(own_key, extent, jnp.float32) * deviation * level
    return jnp.minimum(jnp.maximum(entries, -reach), reach).astype(kind)


def setup_inputs(seed: int = 0) -> dict:
    seeds = jax.random.split(jax.random.key(seed), 14)
    return {
        "resid": centred(seeds[0], (TOKENS, D), 1.0, 6.0, ((0, 512),)),
        "queries": draw_queries(jax.random.fold_in(seeds[13], 71), 0),
        "keys": draw_keys(jax.random.fold_in(seeds[13], 71), 0),
        "values": centred(seeds[3], (TOKENS, KV * HD), 1.0, 6.0, ((0, 64), (1, 8))),
        "log_gates": draw_log_gates(jax.random.fold_in(seeds[13], 71), 0),
        "out_gate": centred(seeds[5], (TOKENS, H * HD), 1.5, 8.0, ((0, 64), (1, 8))),
        "out_weight": centred(seeds[6], (H * HD, D), (H * HD) ** -0.5, 0.125, ((0, 8),)),
        "post_gain": jnp.clip(1.0 + 0.18 * jax.random.normal(seeds[7], (D,), jnp.float32), 0.1, 1.9),
        "pre_gain": jnp.clip(1.0 + 0.18 * jax.random.normal(seeds[8], (D,), jnp.float32), 0.1, 1.9),
        "ffn_gain": jnp.clip(1.0 + 0.18 * jax.random.normal(seeds[9], (D,), jnp.float32), 0.1, 1.9),
        "gate_weight": centred(seeds[10], (D, FF), D ** -0.5, 0.125, ((0, 64), (1, 8))),
        "up_weight": centred(seeds[11], (D, FF), D ** -0.5, 0.125, ((0, 64), (1, 8))),
        "down_weight": centred(seeds[12], (FF, D), FF ** -0.5, 0.078125, ((0, 8), (1, 64))),
    }


EPS = 1e-06
QUERY_BLOCK = 512

def rms_scale(rows, gain):
    mean_sq = lax.optimization_barrier(jnp.mean(rows * rows, axis=-1, keepdims=True))
    return rows * lax.rsqrt(mean_sq + EPS) * gain

def reference(resid, queries, keys, values, log_gates, out_gate, out_weight, post_gain, pre_gain, ffn_gain, gate_weight, up_weight, down_weight):
    group = H // KV
    scale = HD ** (-0.5)
    total = queries.shape[0]

    def one_head(head):
        kv_head = head // group
        q_head = lax.dynamic_slice_in_dim(queries, (head * HD).astype(jnp.int32), HD, 1)
        k_head = lax.dynamic_slice_in_dim(keys, (kv_head * HD).astype(jnp.int32), HD, 1)
        v_head = lax.dynamic_slice_in_dim(values, (kv_head * HD).astype(jnp.int32), HD, 1)
        c_head = lax.dynamic_slice_in_dim(log_gates, head.astype(jnp.int32), 1, 1)[:, 0]
        pieces = []
        for first in range(0, total, QUERY_BLOCK):
            end = min(first + QUERY_BLOCK, total)
            count = end - first
            scores = jnp.dot(q_head[first:end], k_head[:end].T, preferred_element_type=jnp.float32) * scale
            scores = scores + c_head[first:end, None] - c_head[None, :end]
            causal = (first + jnp.arange(count))[:, None] >= jnp.arange(end)[None, :]
            scores = jnp.where(causal, scores, -jnp.inf)
            top = lax.optimization_barrier(jnp.max(scores, axis=1, keepdims=True))
            weights = jnp.exp(scores - top)
            denom = lax.optimization_barrier(jnp.sum(weights, axis=1, keepdims=True))
            pieces.append(jnp.dot(weights.astype(jnp.bfloat16), v_head[:end], preferred_element_type=jnp.float32) / denom)
        return jnp.concatenate(pieces, axis=0)
    attended = lax.map(one_head, jnp.arange(H, dtype=jnp.int32))
    attended = attended.transpose(1, 0, 2).reshape(total, H * HD)
    gated = (attended * jax.nn.sigmoid(out_gate.astype(jnp.float32))).astype(jnp.bfloat16)
    projected = jnp.dot(gated, out_weight, preferred_element_type=jnp.float32)
    mixed = resid.astype(jnp.float32) + rms_scale(projected, post_gain)
    normed = rms_scale(mixed, pre_gain).astype(jnp.bfloat16)
    gate = jnp.dot(normed, gate_weight, preferred_element_type=jnp.float32)
    up = jnp.dot(normed, up_weight, preferred_element_type=jnp.float32)
    hidden = (jax.nn.silu(gate) * up).astype(jnp.bfloat16)
    ffn = jnp.dot(hidden, down_weight, preferred_element_type=jnp.float32)
    return (mixed + rms_scale(ffn, ffn_gain)).astype(jnp.bfloat16)
```

```python
import jax
import jax.numpy as jnp
from jax import lax
from jax.experimental import pallas as pl
from jax.experimental.pallas import tpu as pltpu
from jax.sharding import Mesh
from jax.sharding import PartitionSpec as P

HD = 64
HL = 4
ROWS = 192
QG = 4
ZH = 8 // QG
YS = 8
NB = ZH * YS
TILE = 384
CH = 256
QR = ROWS * HL
KP = 224
OUTR = 72
FFL = 704
GU = 2 * FFL
WC = 2176
EPS = 1e-06
LOW = -1e30
GAP = 56.0

SP = ("zh", "zl", "y")
TP = ("x", "c")
F32 = jnp.float32
BF16 = jnp.bfloat16
NT = (((1,), (1,)), ((), ()))


def pieces(value):
    one = lax.reduce_precision(value, 8, 7)
    rest = value - one
    two = lax.reduce_precision(rest, 8, 7)
    return one, two, rest - two


def kernel_pieces(value):
    one = value.astype(BF16).astype(F32)
    rest = value - one
    two = rest.astype(BF16).astype(F32)
    return one, two, rest - two


def key_payload(keys, values, log_gates):
    k32 = keys.astype(F32)
    norm = jnp.sqrt(jnp.max(jnp.sum(k32 * k32, axis=1))) * 1.01
    parts = jnp.concatenate(pieces(log_gates), axis=1).T
    ones = jnp.ones((3, ROWS), F32)
    last = jnp.full((1, ROWS), norm, F32)
    side = jnp.concatenate([parts, ones, last], axis=0).astype(BF16)
    left = side[:, :128]
    right = jnp.pad(side[:, 128:], ((0, 0), (0, 64)))
    return jnp.concatenate([jnp.concatenate([keys, values], axis=1), left, right], axis=0)


def attention_kernel(pos, kv, q, own, out, kc, vt, qc, acc, ls, ms):
    zh = pos[0]
    zl = pos[1]
    y = pos[2]
    kc[:, 128:256] = jnp.zeros((NB * ROWS, 128), BF16)
    kmax = jnp.zeros((1, 1), F32)
    for b in range(NB):
        base = b * ROWS
        kc[base : base + ROWS, 0:128] = kv[b, 0:ROWS, :]
        left = kv[b, 192:208, :].astype(F32)
        right = kv[b, 208:224, :].astype(F32)
        kc[base : base + 128, 128:144] = left.T.astype(BF16)
        kc[base + 128 : base + ROWS, 128:144] = right.T[0:64].astype(BF16)
        kmax = jnp.maximum(kmax, left[15:16, 0:1])
    for i in range(NB * ROWS // TILE):
        vt[i] = kc[i * TILE : (i + 1) * TILE, 0:128].T[64:128]
    lane = lax.broadcasted_iota(jnp.int32, (ROWS, 128), 1)
    qmax = jnp.zeros((1, 1), F32)
    for j in range(QG):
        block = jnp.where(j > zl, zh * YS + YS - 1, jnp.maximum(zh * YS - 1, 0))
        ends = kv[block, 208:224, :].astype(F32)[:, 63:64]
        for h in range(HL):
            end = ends[h : h + 1] + ends[4 + h : 5 + h] + ends[8 + h : 9 + h]
            ref = jnp.where(j == zl, own[:, h : h + 1], jnp.broadcast_to(end, (ROWS, 1)))
            qh = q[j, :, h * HD : (h + 1) * HD].astype(F32) * 0.125
            norm = jnp.sqrt(jnp.sum(qh * qh, axis=1, keepdims=True))
            qmax = jnp.maximum(qmax, jnp.max(norm, axis=0, keepdims=True))
            one, two, three = kernel_pieces(ref - norm * kmax)
            side = jnp.where((lane == h) | (lane == 4 + h) | (lane == 8 + h), -1.0, 0.0)
            side = jnp.where(lane == 12, one, side)
            side = jnp.where(lane == 13, two, side)
            side = jnp.where(lane == 14, three, side)
            at = slice(h * ROWS, (h + 1) * ROWS)
            qc[j, at, 0:128] = jnp.concatenate([qh, jnp.zeros((ROWS, HD), F32)], axis=1).astype(BF16)
            qc[j, at, 128:256] = side.astype(BF16)
    acc[...] = jnp.zeros(acc.shape, F32)
    ls[...] = jnp.zeros(ls.shape, F32)
    ms[...] = jnp.full(ms.shape, LOW, F32)
    fast = (2.0 * qmax * kmax)[0, 0] <= GAP

    def unit(j, hz, masked, bounded):
        def step(i, none):
            tile = hz * (YS * ROWS // TILE) + i
            kk = kc[pl.ds(pl.multiple_of(tile * TILE, TILE), TILE), :]
            vv = vt[tile]
            for n in range(QR // CH):
                cols = slice(n * CH, (n + 1) * CH)
                s = lax.dot_general(kk, qc[j, cols, :], NT, preferred_element_type=F32)
                if masked:
                    col = n * CH + lax.broadcasted_iota(jnp.int32, (TILE, CH), 1)
                    for h in range(1, HL):
                        col = jnp.where(col >= ROWS, col - ROWS, col)
                    row = i * TILE + lax.broadcasted_iota(jnp.int32, (TILE, CH), 0)
                    s = jnp.where(row <= col + y * ROWS, s, LOW)
                if bounded:
                    w = jnp.exp(s)
                    ls[j, :, cols] += jnp.sum(w.reshape(TILE // 8, 8, CH), axis=0)
                    acc[j, :, cols] += jnp.dot(vv, w.astype(BF16), preferred_element_type=F32)
                else:
                    old = ms[j, 0:1, cols]
                    new = jnp.maximum(old, jnp.max(s, axis=0, keepdims=True))
                    shrink = jnp.exp(old - new)
                    w = jnp.exp(s - new)
                    ms[j, :, cols] = jnp.broadcast_to(new, (8, CH))
                    part = jnp.sum(w.reshape(TILE // 8, 8, CH), axis=0)
                    ls[j, :, cols] = ls[j, :, cols] * shrink + part
                    got = jnp.dot(vv, w.astype(BF16), preferred_element_type=F32)
                    acc[j, :, cols] = acc[j, :, cols] * shrink + got
            return none

        lax.fori_loop(0, YS * ROWS // TILE, step, 0)

    def units(bounded):
        def one(u, none):
            j = u // ZH
            hz = u % ZH
            edge = (hz == zh) & (j == zl)
            whole = (hz < zh) | ((hz == zh) & (j > zl))

            @pl.when(whole)
            def _():
                unit(j, hz, False, bounded)

            @pl.when(edge)
            def _():
                unit(j, hz, True, bounded)

            return none

        lax.fori_loop(0, QG * ZH, one, 0)

    @pl.when(fast)
    def _():
        units(True)
        ms[...] = jnp.zeros(ms.shape, F32)

    @pl.when(jnp.logical_not(fast))
    def _():
        units(False)

    spot = lax.broadcasted_iota(jnp.int32, (8, 256), 1)
    pick = jnp.where((spot >= 140) & (spot <= 142), 1.0, 0.0).astype(BF16)
    line = lax.broadcasted_iota(jnp.int32, (8, QR), 0)
    for j in range(QG):
        shift = lax.dot_general(pick, qc[j], NT, preferred_element_type=F32)[0:1]
        total = jnp.sum(ls[j], axis=0, keepdims=True)
        top = jnp.where(total > 0.0, ms[j, 0:1, :] - shift, LOW)
        stats = jnp.zeros((8, QR), F32)
        for k, part in enumerate(kernel_pieces(total) + kernel_pieces(top)):
            stats = jnp.where(line == k, part, stats)
        out[j, 0:HD, :] = acc[j].astype(BF16)
        out[j, HD:OUTR, :] = stats.astype(BF16)


def attention(pos, kv, q, own):
    vmem = pl.BlockSpec(memory_space=pltpu.VMEM)
    return pl.pallas_call(
        attention_kernel,
        out_shape=jax.ShapeDtypeStruct((QG, OUTR, QR), BF16),
        in_specs=[pl.BlockSpec(memory_space=pltpu.SMEM), vmem, vmem, vmem],
        out_specs=vmem,
        scratch_shapes=[
            pltpu.VMEM((NB * ROWS, 256), BF16),
            pltpu.VMEM((NB * ROWS // TILE, HD, TILE), BF16),
            pltpu.VMEM((QG, QR, 256), BF16),
            pltpu.VMEM((QG, HD, QR), F32),
            pltpu.VMEM((QG, 8, QR), F32),
            pltpu.VMEM((QG, 8, QR), F32),
        ],
        compiler_params=pltpu.CompilerParams(vmem_limit_bytes=48 * 1024 * 1024),
        cost_estimate=pl.CostEstimate(flops=12_000_000_000, bytes_accessed=4_000_000, transcendentals=9_000_000),
        name="attention",
    )(pos, kv, q, own)


def merge_kernel(parts, gates, weight, out):
    tops = []
    sums = []
    for j in range(QG):
        stats = parts[j, HD:OUTR, :].astype(F32)
        sums.append(stats[0:1] + stats[1:2] + stats[2:3])
        tops.append(stats[3:4] + stats[4:5] + stats[5:6])
    top = tops[0]
    for j in range(1, QG):
        top = jnp.maximum(top, tops[j])
    total = jnp.zeros((1, QR), F32)
    mixed = jnp.zeros((HD, QR), F32)
    for j in range(QG):
        scale = jnp.exp(tops[j] - top)
        total = total + sums[j] * scale
        mixed = mixed + parts[j, 0:HD, :].astype(F32) * scale
    rows = (mixed / total).T
    rows = jnp.concatenate([rows[h * ROWS : (h + 1) * ROWS] for h in range(HL)], axis=1)
    gated = (rows * jax.nn.sigmoid(gates[...].astype(F32))).astype(BF16)
    out[...] = jnp.dot(gated, weight[...], preferred_element_type=F32).astype(BF16)


def merge(parts, gates, weight):
    return pl.pallas_call(
        merge_kernel,
        out_shape=jax.ShapeDtypeStruct((ROWS, weight.shape[1]), BF16),
        compiler_params=pltpu.CompilerParams(vmem_limit_bytes=32 * 1024 * 1024),
        cost_estimate=pl.CostEstimate(flops=400_000_000, bytes_accessed=2_000_000, transcendentals=50_000),
        name="merge",
    )(parts, gates, weight)


FC = 512


def ffn_kernel(rows, weights, out, wv, acc, hid, sems):
    count = weights.shape[0] // FC

    def first(k):
        at = (pl.ds(k * FC, FC), pl.ds(0, GU))
        return pltpu.make_async_copy(weights.at[at], wv.at[at], sems.at[k])

    def second(k):
        at = (pl.ds(k * FC, FC), pl.ds(GU, WC - GU))
        return pltpu.make_async_copy(weights.at[at], wv.at[at], sems.at[count + k])

    for k in range(count):
        first(k).start()
    for k in range(count):
        second(k).start()
    for k in range(count):
        first(k).wait()
        part = jnp.dot(
            rows[:, k * FC : (k + 1) * FC],
            wv[k * FC : (k + 1) * FC, 0:GU],
            preferred_element_type=F32,
        )
        if k == 0:
            acc[...] = part
        else:
            acc[...] += part
    gate = acc[:, 0:FFL]
    up = acc[:, FFL:GU]
    hidden = gate / (1.0 + jnp.exp(-gate)) * up
    hid[:, FFL:] = jnp.zeros((ROWS, WC - GU - FFL), BF16)
    hid[:, 0:FFL] = hidden.astype(BF16)
    for k in range(count):
        second(k).wait()
        out[:, k * FC : (k + 1) * FC] = lax.dot_general(
            hid[...], wv[k * FC : (k + 1) * FC, GU:WC], NT, preferred_element_type=F32
        ).astype(BF16)


def ffn(rows, weights):
    wide = weights.shape[0]
    return pl.pallas_call(
        ffn_kernel,
        out_shape=jax.ShapeDtypeStruct((ROWS, wide), BF16),
        in_specs=[pl.BlockSpec(memory_space=pltpu.VMEM), pl.BlockSpec(memory_space=pl.ANY)],
        out_specs=pl.BlockSpec(memory_space=pltpu.VMEM),
        scratch_shapes=[
            pltpu.VMEM((wide, WC), BF16),
            pltpu.VMEM((ROWS, GU), F32),
            pltpu.VMEM((ROWS, WC - GU), BF16),
            pltpu.SemaphoreType.DMA((2 * (wide // FC),)),
        ],
        compiler_params=pltpu.CompilerParams(vmem_limit_bytes=40 * 1024 * 1024),
        cost_estimate=pl.CostEstimate(flops=1_700_000_000, bytes_accessed=10_000_000, transcendentals=140_000),
        name="ffn",
    )(rows, weights)


def copies(value, axis):
    peers = lax.axis_size(axis)
    return lax.all_to_all(jnp.broadcast_to(value[None], (peers, *value.shape)), axis, 0, 0, tiled=True)


def sum_at_owner(value):
    peers = lax.axis_size(TP)
    blocks = value.reshape(peers, value.shape[0] // peers, value.shape[1])
    arrived = lax.all_to_all(blocks, TP, 0, 0, tiled=True)
    return arrived.astype(F32).sum(axis=0)


def rms_scale(rows, gain):
    mean_sq = jnp.mean(rows * rows, axis=-1, keepdims=True)
    return rows * lax.rsqrt(mean_sq + EPS) * gain


def shards(
    resid,
    queries,
    keys,
    values,
    log_gates,
    out_gate,
    out_weight,
    post_gain,
    pre_gain,
    ffn_gain,
    gate_weight,
    up_weight,
    down_weight,
):
    pad = jnp.zeros((gate_weight.shape[0], WC - GU - FFL), BF16)
    packed = jnp.concatenate([gate_weight, up_weight, down_weight.T, pad], axis=1)
    weights = lax.all_gather(packed, SP, axis=0, tiled=True)
    kv = copies(key_payload(keys, values, log_gates), ("zh", "y"))
    q_all = copies(queries, "zl")
    pos = jnp.stack([lax.axis_index("zh"), lax.axis_index("zl"), lax.axis_index("y")]).astype(jnp.int32)
    parts = attention(pos, kv, q_all, log_gates)
    parts = lax.all_to_all(parts, "zl", 0, 0, tiled=True)
    projected = sum_at_owner(merge(parts, out_gate, out_weight))
    mixed = resid.astype(F32) + rms_scale(projected, post_gain)
    normed = rms_scale(mixed, pre_gain).astype(BF16)
    normed_all = lax.all_gather(normed, TP, axis=0, tiled=True)
    total = sum_at_owner(ffn(normed_all, weights))
    return (mixed + rms_scale(total, ffn_gain)).astype(BF16)


def solution(mesh):
    split = Mesh(mesh.devices.reshape(ZH, QG, YS, 4, 2), ("zh", "zl", "y", "x", "c"))
    in_specs = (
        P((*SP, *TP), None),
        P(SP, TP),
        P(SP, TP),
        P(SP, TP),
        P(SP, TP),
        P(SP, TP),
        P(TP, None),
        P(),
        P(),
        P(),
        P(SP, TP),
        P(SP, TP),
        P(TP, SP),
    )
    return jax.shard_map(
        shards, mesh=split, in_specs=in_specs, out_specs=P((*SP, *TP), None), check_vma=False
    )
```

```python
import jax
import jax.numpy as jnp
from jax import lax
from jax.experimental import pallas as pl
from jax.experimental.pallas import tpu as pltpu
from jax.sharding import Mesh
from jax.sharding import PartitionSpec as P

HD = 64
HL = 4
ROWS = 192
QG = 4
ZH = 8 // QG
ZGRID = ((0, 3, 4, 7), (6, 5, 2, 1))
YS = 8
NB = ZH * YS
TILE = 1536
CH = 768
QR = ROWS * HL
KP = 224
OUTR = 72
FFL = 704
GU = 2 * FFL
WC = 2176
EPS = 1e-06
LOW = -1e30
GAP = 56.0

SP = ("z", "y")
TP = ("x", "c")
F32 = jnp.float32
BF16 = jnp.bfloat16
NT = (((1,), (1,)), ((), ()))


def pieces(value):
    one = lax.reduce_precision(value, 8, 7)
    rest = value - one
    two = lax.reduce_precision(rest, 8, 7)
    return one, two, rest - two


def kernel_pieces(value):
    one = value.astype(BF16).astype(F32)
    rest = value - one
    two = rest.astype(BF16).astype(F32)
    return one, two, rest - two


def key_payload(keys, values, log_gates):
    k32 = keys.astype(F32)
    norm = jnp.sqrt(jnp.max(jnp.sum(k32 * k32, axis=1))) * 1.01
    parts = jnp.concatenate(pieces(log_gates), axis=1).T
    ones = jnp.ones((3, ROWS), F32)
    last = jnp.full((1, ROWS), norm, F32)
    side = jnp.concatenate([parts, ones, last], axis=0).astype(BF16)
    left = side[:, :128]
    right = jnp.pad(side[:, 128:], ((0, 0), (0, 64)))
    return jnp.concatenate([jnp.concatenate([keys, values], axis=1), left, right], axis=0)


def grid_z(zh, zl):
    z = jnp.int32(0)
    for a in range(ZH):
        for b in range(QG):
            z = jnp.where((zh == a) & (zl == b), ZGRID[a][b], z)
    return z


def attention_kernel(pos, kv, q, own, out, kc, vt, qt, acc, ls, ms):
    zh = pos[0]
    zl = pos[1]
    y = pos[2]
    mine = grid_z(zh, zl)
    lower = jnp.minimum(grid_z(0, zl), grid_z(1, zl))
    upper = jnp.maximum(grid_z(0, zl), grid_z(1, zl))
    low_at = jnp.where(grid_z(0, zl) == lower, 0, 1)
    kc[:, 128:256] = jnp.zeros((NB * ROWS, 128), BF16)
    kmax = jnp.zeros((1, 1), F32)
    for b in range(NB):
        base = b * ROWS
        kc[base : base + ROWS, 0:128] = kv[b, 0:ROWS, :]
        left = kv[b, 192:208, :].astype(F32)
        right = kv[b, 208:224, :].astype(F32)
        kc[base : base + 128, 128:144] = left.T.astype(BF16)
        kc[base + 128 : base + ROWS, 128:144] = right.T[0:64].astype(BF16)
        kmax = jnp.maximum(kmax, left[15:16, 0:1])
    for i in range(NB * ROWS // TILE):
        vt[i] = kc[i * TILE : (i + 1) * TILE, 0:128].T[64:128]
    head = jnp.zeros((16, QR), jnp.int32)
    col = lax.broadcasted_iota(jnp.int32, (16, QR), 1)
    for h in range(1, HL):
        head = head + jnp.where(col >= h * ROWS, 1, 0)
    line = lax.broadcasted_iota(jnp.int32, (16, QR), 0)
    chosen = jnp.where((line < 3 * HL) & (line % HL == head), -1.0, 0.0)
    qmax = jnp.zeros((1, 1), F32)
    owned = jnp.concatenate([own[h : h + 1, :] for h in range(HL)], axis=1)
    for j in range(QG):
        asked = grid_z(zh, j)
        last = jnp.where(asked > upper, 1 - low_at, low_at)
        ends = kv[last * YS + YS - 1, 208:224, :].astype(F32)[:, 63:64]
        turned = (q[j].astype(F32) * 0.125).T
        turned = jnp.concatenate([turned[h * HD : (h + 1) * HD] for h in range(HL)], axis=1)
        norm = jnp.sqrt(jnp.sum(turned * turned, axis=0, keepdims=True))
        qmax = jnp.maximum(qmax, jnp.max(norm, axis=1, keepdims=True))
        ref = jnp.zeros((1, QR), F32)
        for h in range(HL):
            end = ends[h : h + 1] + ends[4 + h : 5 + h] + ends[8 + h : 9 + h]
            ref = jnp.where(head[0:1] == h, end, ref)
        ref = jnp.where(j == zl, owned, ref)
        one, two, three = kernel_pieces(ref - norm * kmax)
        side = jnp.where(line == 12, one, chosen)
        side = jnp.where(line == 13, two, side)
        side = jnp.where(line == 14, three, side)
        qt[j, 0:HD, :] = turned.astype(BF16)
        qt[j, HD:128, :] = jnp.zeros((128 - HD, QR), BF16)
        qt[j, 128:144, :] = side.astype(BF16)
        qt[j, 144:256, :] = jnp.zeros((112, QR), BF16)
    acc[...] = jnp.zeros(acc.shape, F32)
    ls[...] = jnp.zeros(ls.shape, F32)
    ms[...] = jnp.full(ms.shape, LOW, F32)
    fast = (2.0 * qmax * kmax)[0, 0] <= GAP

    def unit(j, hz, masked, bounded):
        def step(i, none):
            tile = hz * (YS * ROWS // TILE) + i
            kk = kc[pl.ds(pl.multiple_of(tile * TILE, TILE), TILE), :]
            vv = vt[tile]
            for n in range(QR // CH):
                cols = slice(n * CH, (n + 1) * CH)
                s = jnp.dot(kk, qt[j, :, cols], preferred_element_type=F32)
                if masked:
                    col = n * CH + lax.broadcasted_iota(jnp.int32, (TILE, CH), 1)
                    for h in range(1, HL):
                        col = jnp.where(col >= ROWS, col - ROWS, col)
                    row = i * TILE + lax.broadcasted_iota(jnp.int32, (TILE, CH), 0)
                    s = jnp.where(row <= col + y * ROWS, s, LOW)
                if bounded:
                    w = jnp.exp(s)
                    ls[j, :, cols] += jnp.sum(w.reshape(TILE // 8, 8, CH), axis=0)
                    acc[j, :, cols] += jnp.dot(vv, w.astype(BF16), preferred_element_type=F32)
                else:
                    old = ms[j, 0:1, cols]
                    new = jnp.maximum(old, jnp.max(s, axis=0, keepdims=True))
                    shrink = jnp.exp(old - new)
                    w = jnp.exp(s - new)
                    ms[j, :, cols] = jnp.broadcast_to(new, (8, CH))
                    part = jnp.sum(w.reshape(TILE // 8, 8, CH), axis=0)
                    ls[j, :, cols] = ls[j, :, cols] * shrink + part
                    got = jnp.dot(vv, w.astype(BF16), preferred_element_type=F32)
                    acc[j, :, cols] = acc[j, :, cols] * shrink + got
            return none

        lax.fori_loop(0, YS * ROWS // TILE, step, 0)

    def units(bounded):
        def one(u, none):
            j = u // ZH
            hz = u % ZH
            asked = grid_z(zh, j)
            held = grid_z(hz, zl)
            edge = asked == held
            whole = asked > held

            @pl.when(whole)
            def _():
                unit(j, hz, False, bounded)

            @pl.when(edge)
            def _():
                unit(j, hz, True, bounded)

            return none

        lax.fori_loop(0, QG * ZH, one, 0)

    @pl.when(fast)
    def _():
        units(True)
        ms[...] = jnp.zeros(ms.shape, F32)

    @pl.when(jnp.logical_not(fast))
    def _():
        units(False)

    spot = lax.broadcasted_iota(jnp.int32, (8, 256), 1)
    pick = jnp.where((spot >= 140) & (spot <= 142), 1.0, 0.0).astype(BF16)
    line = lax.broadcasted_iota(jnp.int32, (8, QR), 0)
    for j in range(QG):
        shift = jnp.dot(pick, qt[j], preferred_element_type=F32)[0:1]
        total = jnp.sum(ls[j], axis=0, keepdims=True)
        top = jnp.where(total > 0.0, ms[j, 0:1, :] - shift, LOW)
        stats = jnp.zeros((8, QR), F32)
        for k, part in enumerate(kernel_pieces(total) + kernel_pieces(top)):
            stats = jnp.where(line == k, part, stats)
        out[j, 0:HD, :] = acc[j].astype(BF16)
        out[j, HD:OUTR, :] = stats.astype(BF16)


def attention(pos, kv, q, own):
    vmem = pl.BlockSpec(memory_space=pltpu.VMEM)
    return pl.pallas_call(
        attention_kernel,
        out_shape=jax.ShapeDtypeStruct((QG, OUTR, QR), BF16),
        in_specs=[pl.BlockSpec(memory_space=pltpu.SMEM), vmem, vmem, vmem],
        out_specs=vmem,
        scratch_shapes=[
            pltpu.VMEM((NB * ROWS, 256), BF16),
            pltpu.VMEM((NB * ROWS // TILE, HD, TILE), BF16),
            pltpu.VMEM((QG, 256, QR), BF16),
            pltpu.VMEM((QG, HD, QR), F32),
            pltpu.VMEM((QG, 8, QR), F32),
            pltpu.VMEM((QG, 8, QR), F32),
        ],
        compiler_params=pltpu.CompilerParams(vmem_limit_bytes=48 * 1024 * 1024),
        cost_estimate=pl.CostEstimate(flops=12_000_000_000, bytes_accessed=4_000_000, transcendentals=9_000_000),
        name="attention",
    )(pos, kv, q, own.T)


def merge_kernel(parts, gates, weight, out):
    tops = []
    sums = []
    for j in range(QG):
        stats = parts[j, HD:OUTR, :].astype(F32)
        sums.append(stats[0:1] + stats[1:2] + stats[2:3])
        tops.append(stats[3:4] + stats[4:5] + stats[5:6])
    top = tops[0]
    for j in range(1, QG):
        top = jnp.maximum(top, tops[j])
    total = jnp.zeros((1, QR), F32)
    mixed = jnp.zeros((HD, QR), F32)
    for j in range(QG):
        scale = jnp.exp(tops[j] - top)
        total = total + sums[j] * scale
        mixed = mixed + parts[j, 0:HD, :].astype(F32) * scale
    rows = (mixed / total).T
    rows = jnp.concatenate([rows[h * ROWS : (h + 1) * ROWS] for h in range(HL)], axis=1)
    gated = (rows * jax.nn.sigmoid(gates[...].astype(F32))).astype(BF16)
    out[...] = jnp.dot(gated, weight[...], preferred_element_type=F32).astype(BF16)


def merge(parts, gates, weight):
    return pl.pallas_call(
        merge_kernel,
        out_shape=jax.ShapeDtypeStruct((ROWS, weight.shape[1]), BF16),
        compiler_params=pltpu.CompilerParams(vmem_limit_bytes=32 * 1024 * 1024),
        cost_estimate=pl.CostEstimate(flops=400_000_000, bytes_accessed=2_000_000, transcendentals=50_000),
        name="merge",
    )(parts, gates, weight)


FC = 512


def ffn_kernel(rows, weights, out, wv, acc, hid, sems):
    count = weights.shape[0] // FC

    def first(k):
        at = (pl.ds(k * FC, FC), pl.ds(0, GU))
        return pltpu.make_async_copy(weights.at[at], wv.at[at], sems.at[k])

    def second(k):
        at = (pl.ds(k * FC, FC), pl.ds(GU, WC - GU))
        return pltpu.make_async_copy(weights.at[at], wv.at[at], sems.at[count + k])

    for k in range(count):
        first(k).start()
    for k in range(count):
        second(k).start()
    for k in range(count):
        first(k).wait()
        part = jnp.dot(
            rows[:, k * FC : (k + 1) * FC],
            wv[k * FC : (k + 1) * FC, 0:GU],
            preferred_element_type=F32,
        )
        if k == 0:
            acc[...] = part
        else:
            acc[...] += part
    gate = acc[:, 0:FFL]
    up = acc[:, FFL:GU]
    hidden = gate / (1.0 + jnp.exp(-gate)) * up
    hid[:, FFL:] = jnp.zeros((ROWS, WC - GU - FFL), BF16)
    hid[:, 0:FFL] = hidden.astype(BF16)
    for k in range(count):
        second(k).wait()
        out[:, k * FC : (k + 1) * FC] = lax.dot_general(
            hid[...], wv[k * FC : (k + 1) * FC, GU:WC], NT, preferred_element_type=F32
        ).astype(BF16)


def ffn(rows, weights):
    wide = weights.shape[0]
    return pl.pallas_call(
        ffn_kernel,
        out_shape=jax.ShapeDtypeStruct((ROWS, wide), BF16),
        in_specs=[pl.BlockSpec(memory_space=pltpu.VMEM), pl.BlockSpec(memory_space=pltpu.HBM)],
        out_specs=pl.BlockSpec(memory_space=pltpu.VMEM),
        scratch_shapes=[
            pltpu.VMEM((wide, WC), BF16),
            pltpu.VMEM((ROWS, GU), F32),
            pltpu.VMEM((ROWS, WC - GU), BF16),
            pltpu.SemaphoreType.DMA((2 * (wide // FC),)),
        ],
        compiler_params=pltpu.CompilerParams(vmem_limit_bytes=60 * 1024 * 1024),
        cost_estimate=pl.CostEstimate(flops=1_700_000_000, bytes_accessed=10_000_000, transcendentals=140_000),
        name="ffn",
    )(rows, weights)


def copies(value, axis, groups):
    sent = jnp.broadcast_to(value[None], (len(groups[0]), *value.shape))
    return lax.all_to_all(sent, axis, 0, 0, axis_index_groups=groups, tiled=True)


def sum_at_owner(value):
    peers = lax.axis_size(TP)
    blocks = value.reshape(peers, value.shape[0] // peers, value.shape[1])
    arrived = lax.all_to_all(blocks, TP, 0, 0, tiled=True)
    return arrived.astype(F32).sum(axis=0)


def rms_scale(rows, gain):
    mean_sq = jnp.mean(rows * rows, axis=-1, keepdims=True)
    return rows * lax.rsqrt(mean_sq + EPS) * gain


def shards(
    resid,
    queries,
    keys,
    values,
    log_gates,
    out_gate,
    out_weight,
    post_gain,
    pre_gain,
    ffn_gain,
    gate_weight,
    up_weight,
    down_weight,
):
    pad = jnp.zeros((gate_weight.shape[0], WC - GU - FFL), BF16)
    packed = jnp.concatenate([gate_weight, up_weight, down_weight.T, pad], axis=1)
    weights = lax.all_gather(packed, SP, axis=0, tiled=True)
    rows_of = [list(row) for row in ZGRID]
    columns = [[ZGRID[a][b] * YS + y for a in range(ZH) for y in range(YS)] for b in range(QG)]
    kv = copies(key_payload(keys, values, log_gates), SP, columns)
    q_all = copies(queries, "z", rows_of)
    z = lax.axis_index("z")
    zh = sum(jnp.where(z == ZGRID[a][b], a, 0) for a in range(ZH) for b in range(QG))
    zl = sum(jnp.where(z == ZGRID[a][b], b, 0) for a in range(ZH) for b in range(QG))
    pos = jnp.stack([zh, zl, lax.axis_index("y")]).astype(jnp.int32)
    parts = attention(pos, kv, q_all, log_gates)
    parts = lax.all_to_all(parts, "z", 0, 0, axis_index_groups=rows_of, tiled=True)
    projected = sum_at_owner(merge(parts, out_gate, out_weight))
    mixed = resid.astype(F32) + rms_scale(projected, post_gain)
    normed = rms_scale(mixed, pre_gain).astype(BF16)
    normed_all = lax.all_gather(normed, TP, axis=0, tiled=True)
    total = sum_at_owner(ffn(normed_all, weights))
    return (mixed + rms_scale(total, ffn_gain)).astype(BF16)


def solution(mesh):
    split = Mesh(mesh.devices.reshape(8, YS, 4, 2), ("z", "y", "x", "c"))
    in_specs = (
        P((*SP, *TP), None),
        P(SP, TP),
        P(SP, TP),
        P(SP, TP),
        P(SP, TP),
        P(SP, TP),
        P(TP, None),
        P(),
        P(),
        P(),
        P(SP, TP),
        P(SP, TP),
        P(TP, SP),
    )
    return jax.shard_map(
        shards, mesh=split, in_specs=in_specs, out_specs=P((*SP, *TP), None), check_vma=False
    )
```

```python
import jax
import jax.numpy as jnp
from jax import lax
from jax.experimental import pallas as pl
from jax.experimental.pallas import tpu as pltpu
from jax.sharding import Mesh
from jax.sharding import PartitionSpec as P

HD = 64
HL = 4
ROWS = 192
QG = 4
ZH = 8 // QG
ZGRID = ((0, 3, 4, 7), (6, 5, 2, 1))
YS = 8
NB = ZH * YS
TILE = 1536
CH = 768
QR = ROWS * HL
KP = 224
OUTR = 72
FFL = 704
GU = 2 * FFL
WC = 2176
EPS = 1e-06
LOW = -1e30
GAP = 56.0

SP = ("z", "y")
TP = ("x", "c")
F32 = jnp.float32
BF16 = jnp.bfloat16
NT = (((1,), (1,)), ((), ()))


def pieces(value):
    one = lax.reduce_precision(value, 8, 7)
    rest = value - one
    two = lax.reduce_precision(rest, 8, 7)
    return one, two, rest - two


def kernel_pieces(value):
    one = value.astype(BF16).astype(F32)
    rest = value - one
    two = rest.astype(BF16).astype(F32)
    return one, two, rest - two


def key_payload(keys, values, log_gates):
    k32 = keys.astype(F32)
    norm = jnp.sqrt(jnp.max(jnp.sum(k32 * k32, axis=1))) * 1.01
    parts = jnp.concatenate(pieces(log_gates), axis=1).T
    ones = jnp.ones((3, ROWS), F32)
    last = jnp.full((1, ROWS), norm, F32)
    side = jnp.concatenate([parts, ones, last], axis=0).astype(BF16)
    left = side[:, :128]
    right = jnp.pad(side[:, 128:], ((0, 0), (0, 64)))
    return jnp.concatenate([jnp.concatenate([keys, values], axis=1), left, right], axis=0)


def grid_z(zh, zl):
    z = jnp.int32(0)
    for a in range(ZH):
        for b in range(QG):
            z = jnp.where((zh == a) & (zl == b), ZGRID[a][b], z)
    return z


def attention_kernel(pos, kv, q0, q1, q2, q3, own, o0, o1, o2, o3, kc, vt, qt, acc, ls, ms):
    q = (q0, q1, q2, q3)
    out = (o0, o1, o2, o3)
    zh = pos[0]
    zl = pos[1]
    y = pos[2]
    mine = grid_z(zh, zl)
    lower = jnp.minimum(grid_z(0, zl), grid_z(1, zl))
    upper = jnp.maximum(grid_z(0, zl), grid_z(1, zl))
    low_at = jnp.where(grid_z(0, zl) == lower, 0, 1)
    kc[:, 128:256] = jnp.zeros((NB * ROWS, 128), BF16)
    kmax = jnp.zeros((1, 1), F32)
    for b in range(NB):
        base = b * ROWS
        kc[base : base + ROWS, 0:128] = kv[b, 0:ROWS, :]
        left = kv[b, 192:208, :].astype(F32)
        right = kv[b, 208:224, :].astype(F32)
        kc[base : base + 128, 128:144] = left.T.astype(BF16)
        kc[base + 128 : base + ROWS, 128:144] = right.T[0:64].astype(BF16)
        kmax = jnp.maximum(kmax, left[15:16, 0:1])
    for i in range(NB * ROWS // TILE):
        vt[i] = kc[i * TILE : (i + 1) * TILE, 0:128].T[64:128]
    head = jnp.zeros((16, QR), jnp.int32)
    col = lax.broadcasted_iota(jnp.int32, (16, QR), 1)
    for h in range(1, HL):
        head = head + jnp.where(col >= h * ROWS, 1, 0)
    line = lax.broadcasted_iota(jnp.int32, (16, QR), 0)
    chosen = jnp.where((line < 3 * HL) & (line % HL == head), -1.0, 0.0)
    qmax = jnp.zeros((1, 1), F32)
    owned = jnp.concatenate([own[h : h + 1, :] for h in range(HL)], axis=1)
    for j in range(QG):
        asked = grid_z(zh, (zl + QG - j) % QG)
        last = jnp.where(asked > upper, 1 - low_at, low_at)
        ends = kv[last * YS + YS - 1, 208:224, :].astype(F32)[:, 63:64]
        turned = (q[j][...].astype(F32) * 0.125).T
        turned = jnp.concatenate([turned[h * HD : (h + 1) * HD] for h in range(HL)], axis=1)
        norm = jnp.sqrt(jnp.sum(turned * turned, axis=0, keepdims=True))
        qmax = jnp.maximum(qmax, jnp.max(norm, axis=1, keepdims=True))
        ref = jnp.zeros((1, QR), F32)
        for h in range(HL):
            end = ends[h : h + 1] + ends[4 + h : 5 + h] + ends[8 + h : 9 + h]
            ref = jnp.where(head[0:1] == h, end, ref)
        ref = owned if j == 0 else ref
        one, two, three = kernel_pieces(ref - norm * kmax)
        side = jnp.where(line == 12, one, chosen)
        side = jnp.where(line == 13, two, side)
        side = jnp.where(line == 14, three, side)
        qt[j, 0:HD, :] = turned.astype(BF16)
        qt[j, HD:128, :] = jnp.zeros((128 - HD, QR), BF16)
        qt[j, 128:144, :] = side.astype(BF16)
        qt[j, 144:256, :] = jnp.zeros((112, QR), BF16)
    acc[...] = jnp.zeros(acc.shape, F32)
    ls[...] = jnp.zeros(ls.shape, F32)
    ms[...] = jnp.full(ms.shape, LOW, F32)
    fast = (2.0 * qmax * kmax)[0, 0] <= GAP

    def unit(j, hz, masked, bounded):
        def step(i, none):
            tile = hz * (YS * ROWS // TILE) + i
            kk = kc[pl.ds(pl.multiple_of(tile * TILE, TILE), TILE), :]
            vv = vt[tile]
            for n in range(QR // CH):
                cols = slice(n * CH, (n + 1) * CH)
                s = jnp.dot(kk, qt[j, :, cols], preferred_element_type=F32)
                if masked:
                    col = n * CH + lax.broadcasted_iota(jnp.int32, (TILE, CH), 1)
                    for h in range(1, HL):
                        col = jnp.where(col >= ROWS, col - ROWS, col)
                    row = i * TILE + lax.broadcasted_iota(jnp.int32, (TILE, CH), 0)
                    s = jnp.where(row <= col + y * ROWS, s, LOW)
                if bounded:
                    w = jnp.exp(s)
                    ls[j, :, cols] += jnp.sum(w.reshape(TILE // 8, 8, CH), axis=0)
                    acc[j, :, cols] += jnp.dot(vv, w.astype(BF16), preferred_element_type=F32)
                else:
                    old = ms[j, 0:1, cols]
                    new = jnp.maximum(old, jnp.max(s, axis=0, keepdims=True))
                    shrink = jnp.exp(old - new)
                    w = jnp.exp(s - new)
                    ms[j, :, cols] = jnp.broadcast_to(new, (8, CH))
                    part = jnp.sum(w.reshape(TILE // 8, 8, CH), axis=0)
                    ls[j, :, cols] = ls[j, :, cols] * shrink + part
                    got = jnp.dot(vv, w.astype(BF16), preferred_element_type=F32)
                    acc[j, :, cols] = acc[j, :, cols] * shrink + got
            return none

        lax.fori_loop(0, YS * ROWS // TILE, step, 0)

    def units(bounded):
        def one(u, none):
            j = u // ZH
            hz = u % ZH
            asked = grid_z(zh, (zl + QG - j) % QG)
            held = grid_z(hz, zl)
            edge = asked == held
            whole = asked > held

            @pl.when(whole)
            def _():
                unit(j, hz, False, bounded)

            @pl.when(edge)
            def _():
                unit(j, hz, True, bounded)

            return none

        lax.fori_loop(0, QG * ZH, one, 0)

    @pl.when(fast)
    def _():
        units(True)
        ms[...] = jnp.zeros(ms.shape, F32)

    @pl.when(jnp.logical_not(fast))
    def _():
        units(False)

    spot = lax.broadcasted_iota(jnp.int32, (8, 256), 1)
    pick = jnp.where((spot >= 140) & (spot <= 142), 1.0, 0.0).astype(BF16)
    line = lax.broadcasted_iota(jnp.int32, (8, QR), 0)
    for j in range(QG):
        shift = jnp.dot(pick, qt[j], preferred_element_type=F32)[0:1]
        total = jnp.sum(ls[j], axis=0, keepdims=True)
        top = jnp.where(total > 0.0, ms[j, 0:1, :] - shift, LOW)
        stats = jnp.zeros((8, QR), F32)
        for k, part in enumerate(kernel_pieces(total) + kernel_pieces(top)):
            stats = jnp.where(line == k, part, stats)
        out[j][0:HD, :] = acc[j].astype(BF16)
        out[j][HD:OUTR, :] = stats.astype(BF16)


def attention(pos, kv, *rest):
    vmem = pl.BlockSpec(memory_space=pltpu.VMEM)
    return pl.pallas_call(
        attention_kernel,
        out_shape=[jax.ShapeDtypeStruct((OUTR, QR), BF16)] * QG,
        in_specs=[pl.BlockSpec(memory_space=pltpu.SMEM)] + [vmem] * (QG + 2),
        out_specs=[vmem] * QG,
        scratch_shapes=[
            pltpu.VMEM((NB * ROWS, 256), BF16),
            pltpu.VMEM((NB * ROWS // TILE, HD, TILE), BF16),
            pltpu.VMEM((QG, 256, QR), BF16),
            pltpu.VMEM((QG, HD, QR), F32),
            pltpu.VMEM((QG, 8, QR), F32),
            pltpu.VMEM((QG, 8, QR), F32),
        ],
        compiler_params=pltpu.CompilerParams(vmem_limit_bytes=48 * 1024 * 1024),
        cost_estimate=pl.CostEstimate(flops=12_000_000_000, bytes_accessed=4_000_000, transcendentals=9_000_000),
        name="attention",
    )(pos, kv, *rest)


def merge_kernel(p0, p1, p2, p3, gates, weight, out):
    parts = (p0, p1, p2, p3)
    tops = []
    sums = []
    for j in range(QG):
        stats = parts[j][HD:OUTR, :].astype(F32)
        sums.append(stats[0:1] + stats[1:2] + stats[2:3])
        tops.append(stats[3:4] + stats[4:5] + stats[5:6])
    top = tops[0]
    for j in range(1, QG):
        top = jnp.maximum(top, tops[j])
    total = jnp.zeros((1, QR), F32)
    mixed = jnp.zeros((HD, QR), F32)
    for j in range(QG):
        scale = jnp.exp(tops[j] - top)
        total = total + sums[j] * scale
        mixed = mixed + parts[j][0:HD, :].astype(F32) * scale
    rows = (mixed / total).T
    rows = jnp.concatenate([rows[h * ROWS : (h + 1) * ROWS] for h in range(HL)], axis=1)
    gated = (rows * jax.nn.sigmoid(gates[...].astype(F32))).astype(BF16)
    out[...] = jnp.dot(gated, weight[...], preferred_element_type=F32).astype(BF16)


def merge(parts, gates, weight):
    return pl.pallas_call(
        merge_kernel,
        out_shape=jax.ShapeDtypeStruct((ROWS, weight.shape[1]), BF16),
        compiler_params=pltpu.CompilerParams(vmem_limit_bytes=32 * 1024 * 1024),
        cost_estimate=pl.CostEstimate(flops=400_000_000, bytes_accessed=2_000_000, transcendentals=50_000),
        name="merge",
    )(*parts, gates, weight)


FC = 1024
DEEP = 4


def ffn_kernel(rows, weights, out, wv, acc, hid, sems):
    count = weights.shape[0] // FC

    def first(k):
        at = (pl.ds(k * FC, FC), pl.ds(0, GU))
        return pltpu.make_async_copy(weights.at[at], wv.at[at], sems.at[k])

    def second(k):
        at = (pl.ds(k * FC, FC), pl.ds(GU, WC - GU))
        return pltpu.make_async_copy(weights.at[at], wv.at[at], sems.at[count + k])

    moves = [first(k) for k in range(count)] + [second(k) for k in range(count)]
    for k in range(DEEP):
        moves[k].start()

    def arrive(k):
        moves[k].wait()
        if k + DEEP < len(moves):
            moves[k + DEEP].start()

    for k in range(count):
        arrive(k)
        part = jnp.dot(
            rows[:, k * FC : (k + 1) * FC],
            wv[k * FC : (k + 1) * FC, 0:GU],
            preferred_element_type=F32,
        )
        if k == 0:
            acc[...] = part
        else:
            acc[...] += part
    gate = acc[:, 0:FFL]
    up = acc[:, FFL:GU]
    hidden = gate / (1.0 + jnp.exp(-gate)) * up
    hid[:, FFL:] = jnp.zeros((ROWS, WC - GU - FFL), BF16)
    hid[:, 0:FFL] = hidden.astype(BF16)
    for k in range(count):
        arrive(count + k)
        out[:, k * FC : (k + 1) * FC] = lax.dot_general(
            hid[...], wv[k * FC : (k + 1) * FC, GU:WC], NT, preferred_element_type=F32
        ).astype(BF16)


def ffn(rows, weights):
    wide = weights.shape[0]
    return pl.pallas_call(
        ffn_kernel,
        out_shape=jax.ShapeDtypeStruct((ROWS, wide), BF16),
        in_specs=[pl.BlockSpec(memory_space=pltpu.VMEM), pl.BlockSpec(memory_space=pltpu.HBM)],
        out_specs=pl.BlockSpec(memory_space=pltpu.VMEM),
        scratch_shapes=[
            pltpu.VMEM((wide, WC), BF16),
            pltpu.VMEM((ROWS, GU), F32),
            pltpu.VMEM((ROWS, WC - GU), BF16),
            pltpu.SemaphoreType.DMA((2 * (wide // FC),)),
        ],
        compiler_params=pltpu.CompilerParams(vmem_limit_bytes=60 * 1024 * 1024),
        cost_estimate=pl.CostEstimate(flops=1_700_000_000, bytes_accessed=10_000_000, transcendentals=140_000),
        name="ffn",
    )(rows, weights)


def copies(value, axis, groups):
    sent = jnp.broadcast_to(value[None], (len(groups[0]), *value.shape))
    return lax.all_to_all(sent, axis, 0, 0, axis_index_groups=groups, tiled=True)


def sum_at_owner(value):
    peers = lax.axis_size(TP)
    blocks = value.reshape(peers, value.shape[0] // peers, value.shape[1])
    arrived = lax.all_to_all(blocks, TP, 0, 0, tiled=True)
    return arrived.astype(F32).sum(axis=0)


def rms_scale(rows, gain):
    mean_sq = jnp.mean(rows * rows, axis=-1, keepdims=True)
    return rows * lax.rsqrt(mean_sq + EPS) * gain


def shards(
    resid,
    queries,
    keys,
    values,
    log_gates,
    out_gate,
    out_weight,
    post_gain,
    pre_gain,
    ffn_gain,
    gate_weight,
    up_weight,
    down_weight,
):
    def turn(r):
        return [(row[i], row[(i + r) % QG]) for row in ZGRID for i in range(QG)]

    pad = jnp.zeros((gate_weight.shape[0], WC - GU - FFL), BF16)
    packed = jnp.concatenate([gate_weight, up_weight, down_weight.T, pad], axis=1)
    weights = lax.all_gather(packed, SP, axis=0, tiled=True)
    columns = [[ZGRID[a][b] * YS + y for a in range(ZH) for y in range(YS)] for b in range(QG)]
    q_all = [queries] + [lax.ppermute(queries, "z", turn(r)) for r in range(1, QG)]
    kv = copies(key_payload(keys, values, log_gates), SP, columns)
    z = lax.axis_index("z")
    zh = sum(jnp.where(z == ZGRID[a][b], a, 0) for a in range(ZH) for b in range(QG))
    zl = sum(jnp.where(z == ZGRID[a][b], b, 0) for a in range(ZH) for b in range(QG))
    pos = jnp.stack([zh, zl, lax.axis_index("y")]).astype(jnp.int32)
    parts = attention(pos, kv, *q_all, log_gates.T)
    parts = [parts[0]] + [lax.ppermute(parts[r], "z", turn(QG - r)) for r in range(1, QG)]
    projected = sum_at_owner(merge(parts, out_gate, out_weight))
    mixed = resid.astype(F32) + rms_scale(projected, post_gain)
    normed = rms_scale(mixed, pre_gain).astype(BF16)
    normed_all = lax.all_gather(normed, TP, axis=0, tiled=True)
    total = sum_at_owner(ffn(normed_all, weights))
    return (mixed + rms_scale(total, ffn_gain)).astype(BF16)


def solution(mesh):
    split = Mesh(mesh.devices.reshape(8, YS, 4, 2), ("z", "y", "x", "c"))
    in_specs = (
        P((*SP, *TP), None),
        P(SP, TP),
        P(SP, TP),
        P(SP, TP),
        P(SP, TP),
        P(SP, TP),
        P(TP, None),
        P(),
        P(),
        P(),
        P(SP, TP),
        P(SP, TP),
        P(TP, SP),
    )
    return jax.shard_map(
        shards, mesh=split, in_specs=in_specs, out_specs=P((*SP, *TP), None), check_vma=False
    )
```

```python
import jax
import jax.numpy as jnp
from jax import lax
from jax.experimental import pallas as pl
from jax.experimental.pallas import tpu as pltpu
from jax.sharding import Mesh
from jax.sharding import PartitionSpec as P

HD = 64
HL = 4
ROWS = 192
QG = 4
ZH = 8 // QG
ZGRID = ((0, 2, 4, 6), (7, 1, 3, 5))
YS = 8
NB = ZH * YS
TILE = 1536
CH = 768
QR = ROWS * HL
KP = 224
OUTR = 72
FFL = 704
GU = 2 * FFL
WC = 2176
EPS = 1e-06
LOW = -1e30
GAP = 56.0

SP = ("z", "y")
TP = ("x", "c")
F32 = jnp.float32
BF16 = jnp.bfloat16
NT = (((1,), (1,)), ((), ()))


def pieces(value):
    one = lax.reduce_precision(value, 8, 7)
    rest = value - one
    two = lax.reduce_precision(rest, 8, 7)
    return one, two, rest - two


def kernel_pieces(value):
    one = value.astype(BF16).astype(F32)
    rest = value - one
    two = rest.astype(BF16).astype(F32)
    return one, two, rest - two


def key_payload(keys, values, log_gates):
    k32 = keys.astype(F32)
    norm = jnp.sqrt(jnp.max(jnp.sum(k32 * k32, axis=1))) * 1.01
    parts = jnp.concatenate(pieces(log_gates), axis=1).T
    ones = jnp.ones((3, ROWS), F32)
    last = jnp.full((1, ROWS), norm, F32)
    side = jnp.concatenate([parts, ones, last], axis=0).astype(BF16)
    left = side[:, :128]
    right = jnp.pad(side[:, 128:], ((0, 0), (0, 64)))
    return jnp.concatenate([jnp.concatenate([keys, values], axis=1), left, right], axis=0)


def grid_z(zh, zl):
    z = jnp.int32(0)
    for a in range(ZH):
        for b in range(QG):
            z = jnp.where((zh == a) & (zl == b), ZGRID[a][b], z)
    return z


def attention_kernel(pos, kv0, kv1, q0, q1, q2, q3, own, o0, o1, o2, o3, kc, vt, qt, acc, ls, ms):
    kv = (kv0, kv1)
    q = (q0, q1, q2, q3)
    out = (o0, o1, o2, o3)
    zh = pos[0]
    zl = pos[1]
    y = pos[2]
    mine = grid_z(zh, zl)
    theirs = grid_z(1 - zh, zl)
    upper = jnp.maximum(mine, theirs)
    low_at = jnp.where(mine < theirs, 0, 1)
    kc[:, 128:256] = jnp.zeros((NB * ROWS, 128), BF16)
    kmax = jnp.zeros((1, 1), F32)
    for b in range(NB):
        base = b * ROWS
        block = kv[b // YS].at[b % YS]
        kc[base : base + ROWS, 0:128] = block[0:ROWS, :]
        left = block[192:208, :].astype(F32)
        right = block[208:224, :].astype(F32)
        kc[base : base + 128, 128:144] = left.T.astype(BF16)
        kc[base + 128 : base + ROWS, 128:144] = right.T[0:64].astype(BF16)
        kmax = jnp.maximum(kmax, left[15:16, 0:1])
    for i in range(NB * ROWS // TILE):
        vt[i] = kc[i * TILE : (i + 1) * TILE, 0:128].T[64:128]
    head = jnp.zeros((16, QR), jnp.int32)
    col = lax.broadcasted_iota(jnp.int32, (16, QR), 1)
    for h in range(1, HL):
        head = head + jnp.where(col >= h * ROWS, 1, 0)
    line = lax.broadcasted_iota(jnp.int32, (16, QR), 0)
    chosen = jnp.where((line < 3 * HL) & (line % HL == head), -1.0, 0.0)
    qmax = jnp.zeros((1, 1), F32)
    owned = jnp.concatenate([own[h : h + 1, :] for h in range(HL)], axis=1)
    for j in range(QG):
        asked = grid_z(zh, (zl + QG - j) % QG)
        last = jnp.where(asked > upper, 1 - low_at, low_at)
        ends = [rows[YS - 1, 208:224, :].astype(F32)[:, 63:64] for rows in kv]
        ends = jnp.where(last == 0, ends[0], ends[1])
        turned = (q[j][...].astype(F32) * 0.125).T
        turned = jnp.concatenate([turned[h * HD : (h + 1) * HD] for h in range(HL)], axis=1)
        norm = jnp.sqrt(jnp.sum(turned * turned, axis=0, keepdims=True))
        qmax = jnp.maximum(qmax, jnp.max(norm, axis=1, keepdims=True))
        ref = jnp.zeros((1, QR), F32)
        for h in range(HL):
            end = ends[h : h + 1] + ends[4 + h : 5 + h] + ends[8 + h : 9 + h]
            ref = jnp.where(head[0:1] == h, end, ref)
        ref = owned if j == 0 else ref
        one, two, three = kernel_pieces(ref - norm * kmax)
        side = jnp.where(line == 12, one, chosen)
        side = jnp.where(line == 13, two, side)
        side = jnp.where(line == 14, three, side)
        qt[j, 0:HD, :] = turned.astype(BF16)
        qt[j, HD:128, :] = jnp.zeros((128 - HD, QR), BF16)
        qt[j, 128:144, :] = side.astype(BF16)
        qt[j, 144:256, :] = jnp.zeros((112, QR), BF16)
    acc[...] = jnp.zeros(acc.shape, F32)
    ls[...] = jnp.zeros(ls.shape, F32)
    ms[...] = jnp.full(ms.shape, LOW, F32)
    fast = (2.0 * qmax * kmax)[0, 0] <= GAP

    def unit(j, hz, masked, bounded):
        def step(i, none):
            tile = hz * (YS * ROWS // TILE) + i
            kk = kc[pl.ds(pl.multiple_of(tile * TILE, TILE), TILE), :]
            vv = vt[tile]
            for n in range(QR // CH):
                cols = slice(n * CH, (n + 1) * CH)
                s = jnp.dot(kk, qt[j, :, cols], preferred_element_type=F32)
                if masked:
                    col = n * CH + lax.broadcasted_iota(jnp.int32, (TILE, CH), 1)
                    for h in range(1, HL):
                        col = jnp.where(col >= ROWS, col - ROWS, col)
                    row = i * TILE + lax.broadcasted_iota(jnp.int32, (TILE, CH), 0)
                    s = jnp.where(row <= col + y * ROWS, s, LOW)
                if bounded:
                    w = jnp.exp(s)
                    ls[j, :, cols] += jnp.sum(w.reshape(TILE // 8, 8, CH), axis=0)
                    acc[j, :, cols] += jnp.dot(vv, w.astype(BF16), preferred_element_type=F32)
                else:
                    old = ms[j, 0:1, cols]
                    new = jnp.maximum(old, jnp.max(s, axis=0, keepdims=True))
                    shrink = jnp.exp(old - new)
                    w = jnp.exp(s - new)
                    ms[j, :, cols] = jnp.broadcast_to(new, (8, CH))
                    part = jnp.sum(w.reshape(TILE // 8, 8, CH), axis=0)
                    ls[j, :, cols] = ls[j, :, cols] * shrink + part
                    got = jnp.dot(vv, w.astype(BF16), preferred_element_type=F32)
                    acc[j, :, cols] = acc[j, :, cols] * shrink + got
            return none

        lax.fori_loop(0, YS * ROWS // TILE, step, 0)

    def units(bounded):
        def one(u, none):
            j = u // ZH
            hz = u % ZH
            asked = grid_z(zh, (zl + QG - j) % QG)
            edge = u == 0
            whole = asked > jnp.where(hz == 0, mine, theirs)

            @pl.when(whole)
            def _():
                unit(j, hz, False, bounded)

            @pl.when(edge)
            def _():
                unit(j, hz, True, bounded)

            return none

        lax.fori_loop(0, QG * ZH, one, 0)

    @pl.when(fast)
    def _():
        units(True)
        ms[...] = jnp.zeros(ms.shape, F32)

    @pl.when(jnp.logical_not(fast))
    def _():
        units(False)

    spot = lax.broadcasted_iota(jnp.int32, (8, 256), 1)
    pick = jnp.where((spot >= 140) & (spot <= 142), 1.0, 0.0).astype(BF16)
    line = lax.broadcasted_iota(jnp.int32, (8, QR), 0)
    for j in range(QG):
        shift = jnp.dot(pick, qt[j], preferred_element_type=F32)[0:1]
        total = jnp.sum(ls[j], axis=0, keepdims=True)
        top = jnp.where(total > 0.0, ms[j, 0:1, :] - shift, LOW)
        stats = jnp.zeros((8, QR), F32)
        for k, part in enumerate(kernel_pieces(total) + kernel_pieces(top)):
            stats = jnp.where(line == k, part, stats)
        out[j][0:HD, :] = acc[j].astype(BF16)
        out[j][HD:OUTR, :] = stats.astype(BF16)


def attention(pos, *rest):
    vmem = pl.BlockSpec(memory_space=pltpu.VMEM)
    return pl.pallas_call(
        attention_kernel,
        out_shape=[jax.ShapeDtypeStruct((OUTR, QR), BF16)] * QG,
        in_specs=[pl.BlockSpec(memory_space=pltpu.SMEM)] + [vmem] * (QG + 3),
        out_specs=[vmem] * QG,
        scratch_shapes=[
            pltpu.VMEM((NB * ROWS, 256), BF16),
            pltpu.VMEM((NB * ROWS // TILE, HD, TILE), BF16),
            pltpu.VMEM((QG, 256, QR), BF16),
            pltpu.VMEM((QG, HD, QR), F32),
            pltpu.VMEM((QG, 8, QR), F32),
            pltpu.VMEM((QG, 8, QR), F32),
        ],
        compiler_params=pltpu.CompilerParams(vmem_limit_bytes=48 * 1024 * 1024),
        cost_estimate=pl.CostEstimate(flops=12_000_000_000, bytes_accessed=4_000_000, transcendentals=9_000_000),
        name="attention",
    )(pos, *rest)


def merge_kernel(p0, p1, p2, p3, gates, weight, out):
    parts = (p0, p1, p2, p3)
    tops = []
    sums = []
    for j in range(QG):
        stats = parts[j][HD:OUTR, :].astype(F32)
        sums.append(stats[0:1] + stats[1:2] + stats[2:3])
        tops.append(stats[3:4] + stats[4:5] + stats[5:6])
    top = tops[0]
    for j in range(1, QG):
        top = jnp.maximum(top, tops[j])
    total = jnp.zeros((1, QR), F32)
    mixed = jnp.zeros((HD, QR), F32)
    for j in range(QG):
        scale = jnp.exp(tops[j] - top)
        total = total + sums[j] * scale
        mixed = mixed + parts[j][0:HD, :].astype(F32) * scale
    rows = (mixed / total).T
    rows = jnp.concatenate([rows[h * ROWS : (h + 1) * ROWS] for h in range(HL)], axis=1)
    gated = (rows * jax.nn.sigmoid(gates[...].astype(F32))).astype(BF16)
    out[...] = jnp.dot(gated, weight[...], preferred_element_type=F32).astype(BF16)


def merge(parts, gates, weight):
    return pl.pallas_call(
        merge_kernel,
        out_shape=jax.ShapeDtypeStruct((ROWS, weight.shape[1]), BF16),
        compiler_params=pltpu.CompilerParams(vmem_limit_bytes=32 * 1024 * 1024),
        cost_estimate=pl.CostEstimate(flops=400_000_000, bytes_accessed=2_000_000, transcendentals=50_000),
        name="merge",
    )(*parts, gates, weight)


FC = 1024
DEEP = 4


def ffn_kernel(rows, weights, out, wv, acc, hid, sems):
    count = weights.shape[0] // FC

    def first(k):
        at = (pl.ds(k * FC, FC), pl.ds(0, GU))
        return pltpu.make_async_copy(weights.at[at], wv.at[at], sems.at[k])

    def second(k):
        at = (pl.ds(k * FC, FC), pl.ds(GU, WC - GU))
        return pltpu.make_async_copy(weights.at[at], wv.at[at], sems.at[count + k])

    moves = [first(k) for k in range(count)] + [second(k) for k in range(count)]
    for k in range(DEEP):
        moves[k].start()

    def arrive(k):
        moves[k].wait()
        if k + DEEP < len(moves):
            moves[k + DEEP].start()

    for k in range(count):
        arrive(k)
        part = jnp.dot(
            rows[:, k * FC : (k + 1) * FC],
            wv[k * FC : (k + 1) * FC, 0:GU],
            preferred_element_type=F32,
        )
        if k == 0:
            acc[...] = part
        else:
            acc[...] += part
    gate = acc[:, 0:FFL]
    up = acc[:, FFL:GU]
    hidden = gate / (1.0 + jnp.exp(-gate)) * up
    hid[:, FFL:] = jnp.zeros((ROWS, WC - GU - FFL), BF16)
    hid[:, 0:FFL] = hidden.astype(BF16)
    for k in range(count):
        arrive(count + k)
        out[:, k * FC : (k + 1) * FC] = lax.dot_general(
            hid[...], wv[k * FC : (k + 1) * FC, GU:WC], NT, preferred_element_type=F32
        ).astype(BF16)


def ffn(rows, weights):
    wide = weights.shape[0]
    return pl.pallas_call(
        ffn_kernel,
        out_shape=jax.ShapeDtypeStruct((ROWS, wide), BF16),
        in_specs=[pl.BlockSpec(memory_space=pltpu.VMEM), pl.BlockSpec(memory_space=pltpu.HBM)],
        out_specs=pl.BlockSpec(memory_space=pltpu.VMEM),
        scratch_shapes=[
            pltpu.VMEM((wide, WC), BF16),
            pltpu.VMEM((ROWS, GU), F32),
            pltpu.VMEM((ROWS, WC - GU), BF16),
            pltpu.SemaphoreType.DMA((2 * (wide // FC),)),
        ],
        compiler_params=pltpu.CompilerParams(vmem_limit_bytes=60 * 1024 * 1024),
        cost_estimate=pl.CostEstimate(flops=1_700_000_000, bytes_accessed=10_000_000, transcendentals=140_000),
        name="ffn",
    )(rows, weights)


def copies(value, axis):
    sent = jnp.broadcast_to(value[None], (lax.axis_size(axis), *value.shape))
    return lax.all_to_all(sent, axis, 0, 0, tiled=True)


def sum_at_owner(value):
    peers = lax.axis_size(TP)
    blocks = value.reshape(peers, value.shape[0] // peers, value.shape[1])
    arrived = lax.all_to_all(blocks, TP, 0, 0, tiled=True)
    return arrived.astype(F32).sum(axis=0)


def rms_scale(rows, gain):
    mean_sq = jnp.mean(rows * rows, axis=-1, keepdims=True)
    return rows * lax.rsqrt(mean_sq + EPS) * gain


def shards(
    resid,
    queries,
    keys,
    values,
    log_gates,
    out_gate,
    out_weight,
    post_gain,
    pre_gain,
    ffn_gain,
    gate_weight,
    up_weight,
    down_weight,
):
    def turn(r):
        return [(row[i], row[(i + r) % QG]) for row in ZGRID for i in range(QG)]

    pad = jnp.zeros((gate_weight.shape[0], WC - GU - FFL), BF16)
    packed = jnp.concatenate([gate_weight, up_weight, down_weight.T, pad], axis=1)
    weights = lax.all_gather(packed, SP, axis=0, tiled=True)
    q_all = [queries] + [lax.ppermute(queries, "z", turn(r)) for r in range(1, QG)]
    held = copies(key_payload(keys, values, log_gates), "y")
    swap = [pair for column in zip(*ZGRID) for pair in (column, column[::-1])]
    lent = lax.ppermute(held, "z", swap)
    z = lax.axis_index("z")
    zh = sum(jnp.where(z == ZGRID[a][b], a, 0) for a in range(ZH) for b in range(QG))
    zl = sum(jnp.where(z == ZGRID[a][b], b, 0) for a in range(ZH) for b in range(QG))
    pos = jnp.stack([zh, zl, lax.axis_index("y")]).astype(jnp.int32)
    parts = attention(pos, held, lent, *q_all, log_gates.T)
    parts = [parts[0]] + [lax.ppermute(parts[r], "z", turn(QG - r)) for r in range(1, QG)]
    projected = sum_at_owner(merge(parts, out_gate, out_weight))
    mixed = resid.astype(F32) + rms_scale(projected, post_gain)
    normed = rms_scale(mixed, pre_gain).astype(BF16)
    normed_all = lax.all_gather(normed, TP, axis=0, tiled=True)
    total = sum_at_owner(ffn(normed_all, weights))
    return (mixed + rms_scale(total, ffn_gain)).astype(BF16)


def solution(mesh):
    split = Mesh(mesh.devices.reshape(8, YS, 4, 2), ("z", "y", "x", "c"))
    in_specs = (
        P((*SP, *TP), None),
        P(SP, TP),
        P(SP, TP),
        P(SP, TP),
        P(SP, TP),
        P(SP, TP),
        P(TP, None),
        P(),
        P(),
        P(),
        P(SP, TP),
        P(SP, TP),
        P(TP, SP),
    )
    return jax.shard_map(
        shards, mesh=split, in_specs=in_specs, out_specs=P((*SP, *TP), None), check_vma=False
    )
```

```python
import jax
import jax.numpy as jnp
from jax import lax
from jax.experimental import pallas as pl
from jax.experimental.pallas import tpu as pltpu
from jax.sharding import Mesh
from jax.sharding import PartitionSpec as P

HD = 64
HL = 4
ROWS = 192
QG = 4
ZH = 8 // QG
ZGRID = ((0, 2, 4, 6), (7, 1, 3, 5))
YS = 8
NB = ZH * YS
TILE = 1536
CH = 768
QR = ROWS * HL
KP = 224
OUTR = 72
FFL = 704
GU = 2 * FFL
WC = 2176
EPS = 1e-06
TPS = 8
OWN = ROWS // TPS
LOW = -1e30
GAP = 56.0

SP = ("z", "y")
TP = ("x", "c")
F32 = jnp.float32
BF16 = jnp.bfloat16
NT = (((1,), (1,)), ((), ()))


def pieces(value):
    one = lax.reduce_precision(value, 8, 7)
    rest = value - one
    two = lax.reduce_precision(rest, 8, 7)
    return one, two, rest - two


def kernel_pieces(value):
    one = value.astype(BF16).astype(F32)
    rest = value - one
    two = rest.astype(BF16).astype(F32)
    return one, two, rest - two


def key_payload(keys, values, log_gates):
    k32 = keys.astype(F32)
    norm = jnp.sqrt(jnp.max(jnp.sum(k32 * k32, axis=1))) * 1.01
    parts = jnp.concatenate(pieces(log_gates), axis=1).T
    ones = jnp.ones((3, ROWS), F32)
    last = jnp.full((1, ROWS), norm, F32)
    side = jnp.concatenate([parts, ones, last], axis=0).astype(BF16)
    left = side[:, :128]
    right = jnp.pad(side[:, 128:], ((0, 0), (0, 64)))
    return jnp.concatenate([jnp.concatenate([keys, values], axis=1), left, right], axis=0)


def grid_z(zh, zl):
    z = jnp.int32(0)
    for a in range(ZH):
        for b in range(QG):
            z = jnp.where((zh == a) & (zl == b), ZGRID[a][b], z)
    return z


def attention_kernel(pos, kv0, kv1, q0, q1, q2, q3, own, o0, o1, o2, o3, kc, vt, qt, acc, ls, ms):
    kv = (kv0, kv1)
    q = (q0, q1, q2, q3)
    out = (o0, o1, o2, o3)
    zh = pos[0]
    zl = pos[1]
    y = pos[2]
    mine = grid_z(zh, zl)
    theirs = grid_z(1 - zh, zl)
    upper = jnp.maximum(mine, theirs)
    low_at = jnp.where(mine < theirs, 0, 1)
    kc[:, 128:256] = jnp.zeros((NB * ROWS, 128), BF16)
    kmax = jnp.zeros((1, 1), F32)
    for b in range(NB):
        base = b * ROWS
        block = kv[b // YS].at[b % YS]
        kc[base : base + ROWS, 0:128] = block[0:ROWS, :]
        left = block[192:208, :].astype(F32)
        right = block[208:224, :].astype(F32)
        kc[base : base + 128, 128:144] = left.T.astype(BF16)
        kc[base + 128 : base + ROWS, 128:144] = right.T[0:64].astype(BF16)
        kmax = jnp.maximum(kmax, left[15:16, 0:1])
    for i in range(NB * ROWS // TILE):
        vt[i] = kc[i * TILE : (i + 1) * TILE, 0:128].T[64:128]
    head = jnp.zeros((16, QR), jnp.int32)
    col = lax.broadcasted_iota(jnp.int32, (16, QR), 1)
    for h in range(1, HL):
        head = head + jnp.where(col >= h * ROWS, 1, 0)
    line = lax.broadcasted_iota(jnp.int32, (16, QR), 0)
    chosen = jnp.where((line < 3 * HL) & (line % HL == head), -1.0, 0.0)
    qmax = jnp.zeros((1, 1), F32)
    owned = jnp.concatenate([own[h : h + 1, :] for h in range(HL)], axis=1)
    for j in range(QG):
        asked = grid_z(zh, (zl + QG - j) % QG)
        last = jnp.where(asked > upper, 1 - low_at, low_at)
        ends = [rows[YS - 1, 208:224, :].astype(F32)[:, 63:64] for rows in kv]
        ends = jnp.where(last == 0, ends[0], ends[1])
        turned = (q[j][...].astype(F32) * 0.125).T
        turned = jnp.concatenate([turned[h * HD : (h + 1) * HD] for h in range(HL)], axis=1)
        norm = jnp.sqrt(jnp.sum(turned * turned, axis=0, keepdims=True))
        qmax = jnp.maximum(qmax, jnp.max(norm, axis=1, keepdims=True))
        ref = jnp.zeros((1, QR), F32)
        for h in range(HL):
            end = ends[h : h + 1] + ends[4 + h : 5 + h] + ends[8 + h : 9 + h]
            ref = jnp.where(head[0:1] == h, end, ref)
        ref = owned if j == 0 else ref
        one, two, three = kernel_pieces(ref - norm * kmax)
        side = jnp.where(line == 12, one, chosen)
        side = jnp.where(line == 13, two, side)
        side = jnp.where(line == 14, three, side)
        qt[j, 0:HD, :] = turned.astype(BF16)
        qt[j, HD:128, :] = jnp.zeros((128 - HD, QR), BF16)
        qt[j, 128:144, :] = side.astype(BF16)
        qt[j, 144:256, :] = jnp.zeros((112, QR), BF16)
    acc[...] = jnp.zeros(acc.shape, F32)
    ls[...] = jnp.zeros(ls.shape, F32)
    ms[...] = jnp.full(ms.shape, LOW, F32)
    fast = (2.0 * qmax * kmax)[0, 0] <= GAP

    def unit(j, hz, masked, bounded):
        def step(i, none):
            tile = hz * (YS * ROWS // TILE) + i
            kk = kc[pl.ds(pl.multiple_of(tile * TILE, TILE), TILE), :]
            vv = vt[tile]
            for n in range(QR // CH):
                cols = slice(n * CH, (n + 1) * CH)
                s = jnp.dot(kk, qt[j, :, cols], preferred_element_type=F32)
                if masked:
                    col = n * CH + lax.broadcasted_iota(jnp.int32, (TILE, CH), 1)
                    for h in range(1, HL):
                        col = jnp.where(col >= ROWS, col - ROWS, col)
                    row = i * TILE + lax.broadcasted_iota(jnp.int32, (TILE, CH), 0)
                    s = jnp.where(row <= col + y * ROWS, s, LOW)
                if bounded:
                    w = jnp.exp(s)
                    ls[j, :, cols] += jnp.sum(w.reshape(TILE // 8, 8, CH), axis=0)
                    acc[j, :, cols] += jnp.dot(vv, w.astype(BF16), preferred_element_type=F32)
                else:
                    old = ms[j, 0:1, cols]
                    new = jnp.maximum(old, jnp.max(s, axis=0, keepdims=True))
                    shrink = jnp.exp(old - new)
                    w = jnp.exp(s - new)
                    ms[j, :, cols] = jnp.broadcast_to(new, (8, CH))
                    part = jnp.sum(w.reshape(TILE // 8, 8, CH), axis=0)
                    ls[j, :, cols] = ls[j, :, cols] * shrink + part
                    got = jnp.dot(vv, w.astype(BF16), preferred_element_type=F32)
                    acc[j, :, cols] = acc[j, :, cols] * shrink + got
            return none

        lax.fori_loop(0, YS * ROWS // TILE, step, 0)

    def units(bounded):
        def one(u, none):
            j = u // ZH
            hz = u % ZH
            asked = grid_z(zh, (zl + QG - j) % QG)
            edge = u == 0
            whole = asked > jnp.where(hz == 0, mine, theirs)

            @pl.when(whole)
            def _():
                unit(j, hz, False, bounded)

            @pl.when(edge)
            def _():
                unit(j, hz, True, bounded)

            return none

        lax.fori_loop(0, QG * ZH, one, 0)

    @pl.when(fast)
    def _():
        units(True)
        ms[...] = jnp.zeros(ms.shape, F32)

    @pl.when(jnp.logical_not(fast))
    def _():
        units(False)

    spot = lax.broadcasted_iota(jnp.int32, (8, 256), 1)
    pick = jnp.where((spot >= 140) & (spot <= 142), 1.0, 0.0).astype(BF16)
    line = lax.broadcasted_iota(jnp.int32, (8, QR), 0)
    for j in range(QG):
        shift = jnp.dot(pick, qt[j], preferred_element_type=F32)[0:1]
        total = jnp.sum(ls[j], axis=0, keepdims=True)
        top = jnp.where(total > 0.0, ms[j, 0:1, :] - shift, LOW)
        stats = jnp.zeros((8, QR), F32)
        for k, part in enumerate(kernel_pieces(total) + kernel_pieces(top)):
            stats = jnp.where(line == k, part, stats)
        out[j][0:HD, :] = acc[j].astype(BF16)
        out[j][HD:OUTR, :] = stats.astype(BF16)


def attention(pos, *rest):
    vmem = pl.BlockSpec(memory_space=pltpu.VMEM)
    return pl.pallas_call(
        attention_kernel,
        out_shape=[jax.ShapeDtypeStruct((OUTR, QR), BF16)] * QG,
        in_specs=[pl.BlockSpec(memory_space=pltpu.SMEM)] + [vmem] * (QG + 3),
        out_specs=[vmem] * QG,
        scratch_shapes=[
            pltpu.VMEM((NB * ROWS, 256), BF16),
            pltpu.VMEM((NB * ROWS // TILE, HD, TILE), BF16),
            pltpu.VMEM((QG, 256, QR), BF16),
            pltpu.VMEM((QG, HD, QR), F32),
            pltpu.VMEM((QG, 8, QR), F32),
            pltpu.VMEM((QG, 8, QR), F32),
        ],
        compiler_params=pltpu.CompilerParams(vmem_limit_bytes=48 * 1024 * 1024),
        cost_estimate=pl.CostEstimate(flops=12_000_000_000, bytes_accessed=4_000_000, transcendentals=9_000_000),
        name="attention",
    )(pos, *rest)


def by_core(core, rows, mine, theirs, cols):
    low = rows[0 : ROWS // 2].astype(BF16)
    high = rows[ROWS // 2 :].astype(BF16)
    mine[:, cols] = jnp.where(core == 0, low, high)
    theirs[:, cols] = jnp.where(core == 0, high, low)


def merge_kernel(core, p0, p1, p2, p3, gates, weight, mine, theirs):
    parts = (p0, p1, p2, p3)
    tops = []
    sums = []
    for j in range(QG):
        stats = parts[j][HD:OUTR, :].astype(F32)
        sums.append(stats[0:1] + stats[1:2] + stats[2:3])
        tops.append(stats[3:4] + stats[4:5] + stats[5:6])
    top = tops[0]
    for j in range(1, QG):
        top = jnp.maximum(top, tops[j])
    total = jnp.zeros((1, QR), F32)
    mixed = jnp.zeros((HD, QR), F32)
    for j in range(QG):
        scale = jnp.exp(tops[j] - top)
        total = total + sums[j] * scale
        mixed = mixed + parts[j][0:HD, :].astype(F32) * scale
    rows = (mixed / total).T
    rows = jnp.concatenate([rows[h * ROWS : (h + 1) * ROWS] for h in range(HL)], axis=1)
    rows = rows * jax.nn.sigmoid(gates[...].astype(F32))
    order = [x * 2 + c for c in range(2) for x in range(TPS // 2)]
    gated = jnp.concatenate([rows[k * OWN : (k + 1) * OWN] for k in order], axis=0).astype(BF16)
    projected = jnp.dot(gated, weight[...], preferred_element_type=F32)
    by_core(core[0], projected, mine, theirs, slice(None))


def halves(wide):
    return [jax.ShapeDtypeStruct((ROWS // 2, wide), BF16)] * 2


def merge(core, parts, gates, weight):
    vmem = pl.BlockSpec(memory_space=pltpu.VMEM)
    return pl.pallas_call(
        merge_kernel,
        out_shape=halves(weight.shape[1]),
        in_specs=[pl.BlockSpec(memory_space=pltpu.SMEM)] + [vmem] * (QG + 2),
        out_specs=[vmem] * 2,
        compiler_params=pltpu.CompilerParams(vmem_limit_bytes=32 * 1024 * 1024),
        cost_estimate=pl.CostEstimate(flops=400_000_000, bytes_accessed=2_000_000, transcendentals=50_000),
        name="merge",
    )(core, *parts, gates, weight)


FC = 1024
DEEP = 4


def ffn_kernel(core, rows, weights, mine, theirs, wv, acc, hid, sems):
    count = weights.shape[0] // FC

    def first(k):
        at = (pl.ds(k * FC, FC), pl.ds(0, GU))
        return pltpu.make_async_copy(weights.at[at], wv.at[at], sems.at[k])

    def second(k):
        at = (pl.ds(k * FC, FC), pl.ds(GU, WC - GU))
        return pltpu.make_async_copy(weights.at[at], wv.at[at], sems.at[count + k])

    moves = [first(k) for k in range(count)] + [second(k) for k in range(count)]
    for k in range(DEEP):
        moves[k].start()

    def arrive(k):
        moves[k].wait()
        if k + DEEP < len(moves):
            moves[k + DEEP].start()

    for k in range(count):
        arrive(k)
        part = jnp.dot(
            rows[:, k * FC : (k + 1) * FC],
            wv[k * FC : (k + 1) * FC, 0:GU],
            preferred_element_type=F32,
        )
        if k == 0:
            acc[...] = part
        else:
            acc[...] += part
    gate = acc[:, 0:FFL]
    up = acc[:, FFL:GU]
    hidden = gate / (1.0 + jnp.exp(-gate)) * up
    hid[:, FFL:] = jnp.zeros((ROWS, WC - GU - FFL), BF16)
    hid[:, 0:FFL] = hidden.astype(BF16)
    for k in range(count):
        arrive(count + k)
        part = lax.dot_general(
            hid[...], wv[k * FC : (k + 1) * FC, GU:WC], NT, preferred_element_type=F32
        )
        by_core(core[0], part, mine, theirs, slice(k * FC, (k + 1) * FC))


def ffn(core, rows, weights):
    wide = weights.shape[0]
    vmem = pl.BlockSpec(memory_space=pltpu.VMEM)
    return pl.pallas_call(
        ffn_kernel,
        out_shape=halves(wide),
        in_specs=[pl.BlockSpec(memory_space=pltpu.SMEM), vmem, pl.BlockSpec(memory_space=pltpu.HBM)],
        out_specs=[vmem] * 2,
        scratch_shapes=[
            pltpu.VMEM((wide, WC), BF16),
            pltpu.VMEM((ROWS, GU), F32),
            pltpu.VMEM((ROWS, WC - GU), BF16),
            pltpu.SemaphoreType.DMA((2 * (wide // FC),)),
        ],
        compiler_params=pltpu.CompilerParams(vmem_limit_bytes=55 * 1024 * 1024),
        cost_estimate=pl.CostEstimate(flops=1_700_000_000, bytes_accessed=10_000_000, transcendentals=140_000),
        name="ffn",
    )(core, rows, weights)


def copies(value, axis):
    sent = jnp.broadcast_to(value[None], (lax.axis_size(axis), *value.shape))
    return lax.all_to_all(sent, axis, 0, 0, tiled=True)


def sum_at_owner(mine, theirs):
    given = lax.ppermute(theirs, "c", [(0, 1), (1, 0)])
    both = (mine.astype(F32) + given.astype(F32)).astype(BF16)
    blocks = both.reshape(TPS // 2, OWN, both.shape[1])
    arrived = lax.all_to_all(blocks, "x", 0, 0, tiled=True)
    return arrived.astype(F32).sum(axis=0)


def rms_scale(rows, gain):
    mean_sq = jnp.mean(rows * rows, axis=-1, keepdims=True)
    return rows * lax.rsqrt(mean_sq + EPS) * gain


def shards(
    resid,
    queries,
    keys,
    values,
    log_gates,
    out_gate,
    out_weight,
    post_gain,
    pre_gain,
    ffn_gain,
    gate_weight,
    up_weight,
    down_weight,
):
    def turn(r):
        return [(row[i], row[(i + r) % QG]) for row in ZGRID for i in range(QG)]

    pad = jnp.zeros((gate_weight.shape[0], WC - GU - FFL), BF16)
    packed = jnp.concatenate([gate_weight, up_weight, down_weight.T, pad], axis=1)
    weights = lax.all_gather(packed, SP, axis=0, tiled=True)
    q_all = [queries] + [lax.ppermute(queries, "z", turn(r)) for r in range(1, QG)]
    held = copies(key_payload(keys, values, log_gates), "y")
    swap = [pair for column in zip(*ZGRID) for pair in (column, column[::-1])]
    lent = lax.ppermute(held, "z", swap)
    z = lax.axis_index("z")
    zh = sum(jnp.where(z == ZGRID[a][b], a, 0) for a in range(ZH) for b in range(QG))
    zl = sum(jnp.where(z == ZGRID[a][b], b, 0) for a in range(ZH) for b in range(QG))
    pos = jnp.stack([zh, zl, lax.axis_index("y")]).astype(jnp.int32)
    parts = attention(pos, held, lent, *q_all, log_gates.T)
    parts = [parts[0]] + [lax.ppermute(parts[r], "z", turn(QG - r)) for r in range(1, QG)]
    core = lax.axis_index("c").astype(jnp.int32)[None]
    projected = sum_at_owner(*merge(core, parts, out_gate, out_weight))
    mixed = resid.astype(F32) + rms_scale(projected, post_gain)
    normed = rms_scale(mixed, pre_gain).astype(BF16)
    along = copies(normed, "x").reshape(ROWS // 2, -1)
    normed_all = lax.all_gather(along, "c", axis=0, tiled=True)
    total = sum_at_owner(*ffn(core, normed_all, weights))
    return (mixed + rms_scale(total, ffn_gain)).astype(BF16)


def solution(mesh):
    split = Mesh(mesh.devices.reshape(8, YS, 4, 2), ("z", "y", "x", "c"))
    in_specs = (
        P((*SP, *TP), None),
        P(SP, TP),
        P(SP, TP),
        P(SP, TP),
        P(SP, TP),
        P(SP, TP),
        P(TP, None),
        P(),
        P(),
        P(),
        P(SP, TP),
        P(SP, TP),
        P(TP, SP),
    )
    return jax.shard_map(
        shards, mesh=split, in_specs=in_specs, out_specs=P((*SP, *TP), None), check_vma=False
    )
```

```python
import jax
import jax.numpy as jnp
from jax import lax
from jax.experimental import pallas as pl
from jax.experimental.pallas import tpu as pltpu
from jax.sharding import Mesh
from jax.sharding import PartitionSpec as P

HD = 64
HL = 4
ROWS = 192
QG = 4
ZH = 8 // QG
ZGRID = ((0, 2, 4, 6), (7, 1, 3, 5))
YS = 8
NB = ZH * YS
TILE = 1536
CH = 768
QR = ROWS * HL
KP = 224
OUTR = 72
FFL = 704
GU = 2 * FFL
WC = 2176
EPS = 1e-06
TPS = 8
OWN = ROWS // TPS
LOW = -1e30
GAP = 56.0

SP = ("z", "y")
TP = ("x", "c")
F32 = jnp.float32
BF16 = jnp.bfloat16
NT = (((1,), (1,)), ((), ()))


def kernel_pieces(value):
    one = value.astype(BF16).astype(F32)
    rest = value - one
    two = rest.astype(BF16).astype(F32)
    return one, two, rest - two


def payload_kernel(keys, values, gates, out):
    k32 = keys[...].astype(F32)
    norm = jnp.max(jnp.sum(k32 * k32, axis=0, keepdims=True), axis=1, keepdims=True)
    norm = jnp.sqrt(norm) * 1.01
    rows = jnp.concatenate([k32, values[...].astype(F32)], axis=0).T.astype(BF16)
    line = lax.broadcasted_iota(jnp.int32, (16, ROWS), 0)
    side = jnp.concatenate([*kernel_pieces(gates[...]), jnp.ones((HL, ROWS), F32)], axis=0)
    side = jnp.where(line == 15, norm, side)
    left = side[:, 0:128].astype(BF16)
    right = jnp.concatenate([side[:, 128:], jnp.zeros((16, 64), F32)], axis=1).astype(BF16)
    for n in range(YS):
        out[n, 0:ROWS, :] = rows
        out[n, ROWS : ROWS + 16, :] = left
        out[n, ROWS + 16 : KP, :] = right


def payload(keys, values, gates):
    return pl.pallas_call(
        payload_kernel,
        out_shape=jax.ShapeDtypeStruct((YS, KP, 128), BF16),
        cost_estimate=pl.CostEstimate(flops=100_000, bytes_accessed=500_000, transcendentals=0),
        name="payload",
    )(keys, values, gates)


def grid_z(zh, zl):
    z = jnp.int32(0)
    for a in range(ZH):
        for b in range(QG):
            z = jnp.where((zh == a) & (zl == b), ZGRID[a][b], z)
    return z


def attention_kernel(pos, kv0, kv1, q0, q1, q2, q3, o0, o1, o2, o3, kc, vt, qt, acc, ls, ms):
    kv = (kv0, kv1)
    q = (q0, q1, q2, q3)
    out = (o0, o1, o2, o3)
    zh = pos[0]
    zl = pos[1]
    y = pos[2]
    mine = grid_z(zh, zl)
    theirs = grid_z(1 - zh, zl)
    upper = jnp.maximum(mine, theirs)
    low_at = jnp.where(mine < theirs, 0, 1)
    kc[:, 128:256] = jnp.zeros((NB * ROWS, 128), BF16)
    kmax = jnp.zeros((1, 1), F32)
    for b in range(NB):
        base = b * ROWS
        block = kv[b // YS].at[b % YS]
        kc[base : base + ROWS, 0:128] = block[0:ROWS, :]
        left = block[192:208, :].astype(F32)
        right = block[208:224, :].astype(F32)
        kc[base : base + 128, 128:144] = left.T.astype(BF16)
        kc[base + 128 : base + ROWS, 128:144] = right.T[0:64].astype(BF16)
        kmax = jnp.maximum(kmax, left[15:16, 0:1])
    for i in range(NB * ROWS // TILE):
        vt[i] = kc[i * TILE : (i + 1) * TILE, 0:128].T[64:128]
    head = jnp.zeros((16, QR), jnp.int32)
    col = lax.broadcasted_iota(jnp.int32, (16, QR), 1)
    for h in range(1, HL):
        head = head + jnp.where(col >= h * ROWS, 1, 0)
    line = lax.broadcasted_iota(jnp.int32, (16, QR), 0)
    chosen = jnp.where((line < 3 * HL) & (line % HL == head), -1.0, 0.0)
    qmax = jnp.zeros((1, 1), F32)
    left = kv0[y, ROWS : ROWS + 16, :].astype(F32)
    right = kv0[y, ROWS + 16 : KP, :].astype(F32)[:, 0:64]
    owned = jnp.concatenate([left, right], axis=1)
    owned = owned[0:4] + owned[4:8] + owned[8:12]
    owned = jnp.concatenate([owned[h : h + 1] for h in range(HL)], axis=1)
    for j in range(QG):
        asked = grid_z(zh, (zl + QG - j) % QG)
        last = jnp.where(asked > upper, 1 - low_at, low_at)
        ends = [rows[YS - 1, 208:224, :].astype(F32)[:, 63:64] for rows in kv]
        ends = jnp.where(last == 0, ends[0], ends[1])
        turned = q[j][...].astype(F32).T
        turned = jnp.concatenate([turned[h * HD : (h + 1) * HD] for h in range(HL)], axis=1)
        norm = jnp.sqrt(jnp.sum(turned * turned, axis=0, keepdims=True))
        qmax = jnp.maximum(qmax, jnp.max(norm, axis=1, keepdims=True))
        ref = jnp.zeros((1, QR), F32)
        for h in range(HL):
            end = ends[h : h + 1] + ends[4 + h : 5 + h] + ends[8 + h : 9 + h]
            ref = jnp.where(head[0:1] == h, end, ref)
        ref = owned if j == 0 else ref
        one, two, three = kernel_pieces(ref - norm * kmax)
        side = jnp.where(line == 12, one, chosen)
        side = jnp.where(line == 13, two, side)
        side = jnp.where(line == 14, three, side)
        qt[j, 0:HD, :] = turned.astype(BF16)
        qt[j, HD:128, :] = jnp.zeros((128 - HD, QR), BF16)
        qt[j, 128:144, :] = side.astype(BF16)
        qt[j, 144:256, :] = jnp.zeros((112, QR), BF16)
    acc[...] = jnp.zeros(acc.shape, F32)
    ls[...] = jnp.zeros(ls.shape, F32)
    ms[...] = jnp.full(ms.shape, LOW, F32)
    fast = (2.0 * qmax * kmax)[0, 0] <= GAP

    def unit(j, hz, masked, bounded):
        def step(i, none):
            tile = hz * (YS * ROWS // TILE) + i
            kk = kc[pl.ds(pl.multiple_of(tile * TILE, TILE), TILE), :]
            vv = vt[tile]
            for n in range(QR // CH):
                cols = slice(n * CH, (n + 1) * CH)
                s = jnp.dot(kk, qt[j, :, cols], preferred_element_type=F32)
                if masked:
                    col = n * CH + lax.broadcasted_iota(jnp.int32, (TILE, CH), 1)
                    for h in range(1, HL):
                        col = jnp.where(col >= ROWS, col - ROWS, col)
                    row = i * TILE + lax.broadcasted_iota(jnp.int32, (TILE, CH), 0)
                    s = jnp.where(row <= col + y * ROWS, s, LOW)
                if bounded:
                    w = jnp.exp(s)
                    ls[j, :, cols] += jnp.sum(w.reshape(TILE // 8, 8, CH), axis=0)
                    acc[j, :, cols] += jnp.dot(vv, w.astype(BF16), preferred_element_type=F32)
                else:
                    old = ms[j, 0:1, cols]
                    new = jnp.maximum(old, jnp.max(s, axis=0, keepdims=True))
                    shrink = jnp.exp(old - new)
                    w = jnp.exp(s - new)
                    ms[j, :, cols] = jnp.broadcast_to(new, (8, CH))
                    part = jnp.sum(w.reshape(TILE // 8, 8, CH), axis=0)
                    ls[j, :, cols] = ls[j, :, cols] * shrink + part
                    got = jnp.dot(vv, w.astype(BF16), preferred_element_type=F32)
                    acc[j, :, cols] = acc[j, :, cols] * shrink + got
            return none

        lax.fori_loop(0, YS * ROWS // TILE, step, 0)

    def units(bounded):
        def one(u, none):
            j = u // ZH
            hz = u % ZH
            asked = grid_z(zh, (zl + QG - j) % QG)
            edge = u == 0
            whole = asked > jnp.where(hz == 0, mine, theirs)

            @pl.when(whole)
            def _():
                unit(j, hz, False, bounded)

            @pl.when(edge)
            def _():
                unit(j, hz, True, bounded)

            return none

        lax.fori_loop(0, QG * ZH, one, 0)

    @pl.when(fast)
    def _():
        units(True)
        ms[...] = jnp.zeros(ms.shape, F32)

    @pl.when(jnp.logical_not(fast))
    def _():
        units(False)

    spot = lax.broadcasted_iota(jnp.int32, (8, 256), 1)
    pick = jnp.where((spot >= 140) & (spot <= 142), 1.0, 0.0).astype(BF16)
    line = lax.broadcasted_iota(jnp.int32, (8, QR), 0)
    for j in range(QG):
        shift = jnp.dot(pick, qt[j], preferred_element_type=F32)[0:1]
        total = jnp.sum(ls[j], axis=0, keepdims=True)
        top = jnp.where(total > 0.0, ms[j, 0:1, :] - shift, LOW)
        stats = jnp.zeros((8, QR), F32)
        for k, part in enumerate(kernel_pieces(total) + kernel_pieces(top)):
            stats = jnp.where(line == k, part, stats)
        out[j][0:HD, :] = acc[j].astype(BF16)
        out[j][HD:OUTR, :] = stats.astype(BF16)


def attention(pos, *rest):
    vmem = pl.BlockSpec(memory_space=pltpu.VMEM)
    return pl.pallas_call(
        attention_kernel,
        out_shape=[jax.ShapeDtypeStruct((OUTR, QR), BF16)] * QG,
        in_specs=[pl.BlockSpec(memory_space=pltpu.SMEM)] + [vmem] * (QG + 2),
        out_specs=[vmem] * QG,
        scratch_shapes=[
            pltpu.VMEM((NB * ROWS, 256), BF16),
            pltpu.VMEM((NB * ROWS // TILE, HD, TILE), BF16),
            pltpu.VMEM((QG, 256, QR), BF16),
            pltpu.VMEM((QG, HD, QR), F32),
            pltpu.VMEM((QG, 8, QR), F32),
            pltpu.VMEM((QG, 8, QR), F32),
        ],
        compiler_params=pltpu.CompilerParams(vmem_limit_bytes=48 * 1024 * 1024),
        cost_estimate=pl.CostEstimate(flops=12_000_000_000, bytes_accessed=4_000_000, transcendentals=9_000_000),
        name="attention",
    )(pos, *rest)


def by_core(core, rows, mine, theirs, cols):
    low = rows[0 : ROWS // 2].astype(BF16)
    high = rows[ROWS // 2 :].astype(BF16)
    mine[:, cols] = jnp.where(core == 0, low, high)
    theirs[:, cols] = jnp.where(core == 0, high, low)


def merge_kernel(core, p0, p1, p2, p3, gates, weight, mine, theirs):
    parts = (p0, p1, p2, p3)
    tops = []
    sums = []
    for j in range(QG):
        stats = parts[j][HD:OUTR, :].astype(F32)
        sums.append(stats[0:1] + stats[1:2] + stats[2:3])
        tops.append(jnp.where(sums[j] > 0.0, stats[3:4] + stats[4:5] + stats[5:6], LOW))
    top = tops[0]
    for j in range(1, QG):
        top = jnp.maximum(top, tops[j])
    total = jnp.zeros((1, QR), F32)
    mixed = jnp.zeros((HD, QR), F32)
    for j in range(QG):
        scale = jnp.exp(tops[j] - top)
        total = total + sums[j] * scale
        mixed = mixed + parts[j][0:HD, :].astype(F32) * scale
    rows = (mixed / total).T
    rows = jnp.concatenate([rows[h * ROWS : (h + 1) * ROWS] for h in range(HL)], axis=1)
    rows = rows * jax.nn.sigmoid(gates[...].astype(F32))
    order = [x * 2 + c for c in range(2) for x in range(TPS // 2)]
    gated = jnp.concatenate([rows[k * OWN : (k + 1) * OWN] for k in order], axis=0).astype(BF16)
    projected = jnp.dot(gated, weight[...], preferred_element_type=F32)
    by_core(core[0], projected, mine, theirs, slice(None))


def halves(wide):
    return [jax.ShapeDtypeStruct((ROWS // 2, wide), BF16)] * 2


def merge(core, parts, gates, weight):
    vmem = pl.BlockSpec(memory_space=pltpu.VMEM)
    return pl.pallas_call(
        merge_kernel,
        out_shape=halves(weight.shape[1]),
        in_specs=[pl.BlockSpec(memory_space=pltpu.SMEM)] + [vmem] * (QG + 2),
        out_specs=[vmem] * 2,
        compiler_params=pltpu.CompilerParams(vmem_limit_bytes=32 * 1024 * 1024),
        cost_estimate=pl.CostEstimate(flops=400_000_000, bytes_accessed=2_000_000, transcendentals=50_000),
        name="merge",
    )(core, *parts, gates, weight)


FC = 1024
DEEP = 4


def ffn_kernel(core, rows, weights, mine, theirs, wv, acc, hid, sems):
    count = weights.shape[0] // FC

    def first(k):
        at = (pl.ds(k * FC, FC), pl.ds(0, GU))
        return pltpu.make_async_copy(weights.at[at], wv.at[at], sems.at[k])

    def second(k):
        at = (pl.ds(k * FC, FC), pl.ds(GU, WC - GU))
        return pltpu.make_async_copy(weights.at[at], wv.at[at], sems.at[count + k])

    moves = [first(k) for k in range(count)] + [second(k) for k in range(count)]
    for k in range(DEEP):
        moves[k].start()

    def arrive(k):
        moves[k].wait()
        if k + DEEP < len(moves):
            moves[k + DEEP].start()

    for k in range(count):
        arrive(k)
        part = jnp.dot(
            rows[:, k * FC : (k + 1) * FC],
            wv[k * FC : (k + 1) * FC, 0:GU],
            preferred_element_type=F32,
        )
        if k == 0:
            acc[...] = part
        else:
            acc[...] += part
    gate = acc[:, 0:FFL]
    up = acc[:, FFL:GU]
    hidden = gate / (1.0 + jnp.exp(-gate)) * up
    hid[:, FFL:] = jnp.zeros((ROWS, WC - GU - FFL), BF16)
    hid[:, 0:FFL] = hidden.astype(BF16)
    for k in range(count):
        arrive(count + k)
        part = lax.dot_general(
            hid[...], wv[k * FC : (k + 1) * FC, GU:WC], NT, preferred_element_type=F32
        )
        by_core(core[0], part, mine, theirs, slice(k * FC, (k + 1) * FC))


def ffn(core, rows, weights):
    wide = weights.shape[0]
    vmem = pl.BlockSpec(memory_space=pltpu.VMEM)
    return pl.pallas_call(
        ffn_kernel,
        out_shape=halves(wide),
        in_specs=[pl.BlockSpec(memory_space=pltpu.SMEM), vmem, pl.BlockSpec(memory_space=pltpu.HBM)],
        out_specs=[vmem] * 2,
        scratch_shapes=[
            pltpu.VMEM((wide, WC), BF16),
            pltpu.VMEM((ROWS, GU), F32),
            pltpu.VMEM((ROWS, WC - GU), BF16),
            pltpu.SemaphoreType.DMA((2 * (wide // FC),)),
        ],
        compiler_params=pltpu.CompilerParams(vmem_limit_bytes=55 * 1024 * 1024),
        cost_estimate=pl.CostEstimate(flops=1_700_000_000, bytes_accessed=10_000_000, transcendentals=140_000),
        name="ffn",
    )(core, rows, weights)


def copies(value, axis):
    sent = jnp.broadcast_to(value[None], (lax.axis_size(axis), *value.shape))
    return lax.all_to_all(sent, axis, 0, 0, tiled=True)


def sum_at_owner(mine, theirs):
    given = lax.ppermute(theirs, "c", [(0, 1), (1, 0)])
    both = (mine.astype(F32) + given.astype(F32)).astype(BF16)
    blocks = both.reshape(TPS // 2, OWN, both.shape[1])
    arrived = lax.all_to_all(blocks, "x", 0, 0, tiled=True)
    return arrived.astype(F32).sum(axis=0)


def rms_scale(rows, gain):
    mean_sq = jnp.mean(rows * rows, axis=-1, keepdims=True)
    return rows * lax.rsqrt(mean_sq + EPS) * gain


def shards(
    resid,
    queries,
    keys,
    values,
    log_gates,
    out_gate,
    out_weight,
    post_gain,
    pre_gain,
    ffn_gain,
    gate_weight,
    up_weight,
    down_weight,
):
    pairs = [(row, i, (i + r) % QG, r) for row in ZGRID for i in range(QG) for r in range(1, QG)]
    partner = {a: b for column in zip(*ZGRID) for a, b in (column, column[::-1])}
    asks = [(row[i], row[k], r) for row, i, k, r in pairs if row[i] > min(row[k], partner[row[k]])]

    def ask(r):
        return [(q, k) for q, k, turn in asks if turn == r]

    def answer(r):
        return [(k, q) for q, k, turn in asks if turn == r]

    swap = [(partner[d], d) for row in ZGRID for d in row if max(row) > partner[d]]
    pad = jnp.zeros((gate_weight.shape[0], WC - GU - FFL), BF16)
    packed = jnp.concatenate([gate_weight, up_weight, down_weight.T, pad], axis=1)
    weights = lax.all_gather(packed, SP, axis=0, tiled=True)
    scaled = queries * jnp.asarray(HD**-0.5, BF16)
    q_all = [scaled] + [lax.ppermute(scaled, "z", ask(r)) for r in range(1, QG)]
    held = lax.all_to_all(payload(keys.T, values.T, log_gates.T), "y", 0, 0, tiled=True)
    lent = lax.ppermute(held, "z", swap)
    z = lax.axis_index("z")
    zh = sum(jnp.where(z == ZGRID[a][b], a, 0) for a in range(ZH) for b in range(QG))
    zl = sum(jnp.where(z == ZGRID[a][b], b, 0) for a in range(ZH) for b in range(QG))
    pos = jnp.stack([zh, zl, lax.axis_index("y")]).astype(jnp.int32)
    parts = attention(pos, held, lent, *q_all)
    parts = [parts[0]] + [lax.ppermute(parts[r], "z", answer(r)) for r in range(1, QG)]
    core = lax.axis_index("c").astype(jnp.int32)[None]
    projected = sum_at_owner(*merge(core, parts, out_gate, out_weight))
    mixed = resid.astype(F32) + rms_scale(projected, post_gain)
    normed = rms_scale(mixed, pre_gain).astype(BF16)
    along = copies(normed, "x").reshape(ROWS // 2, -1)
    normed_all = lax.all_gather(along, "c", axis=0, tiled=True)
    total = sum_at_owner(*ffn(core, normed_all, weights))
    return (mixed + rms_scale(total, ffn_gain)).astype(BF16)


def solution(mesh):
    split = Mesh(mesh.devices.reshape(8, YS, 4, 2), ("z", "y", "x", "c"))
    in_specs = (
        P((*SP, *TP), None),
        P(SP, TP),
        P(SP, TP),
        P(SP, TP),
        P(SP, TP),
        P(SP, TP),
        P(TP, None),
        P(),
        P(),
        P(),
        P(SP, TP),
        P(SP, TP),
        P(TP, SP),
    )
    return jax.shard_map(
        shards, mesh=split, in_specs=in_specs, out_specs=P((*SP, *TP), None), check_vma=False
    )
```

```python
import jax
import jax.numpy as jnp
from jax import lax
from jax.experimental import pallas as pl
from jax.experimental.pallas import tpu as pltpu
from jax.sharding import Mesh
from jax.sharding import PartitionSpec as P

HD = 64
HL = 4
ROWS = 192
QG = 4
ZH = 8 // QG
ZGRID = ((0, 2, 4, 6), (7, 1, 3, 5))
YS = 8
NB = ZH * YS
TILE = 1536
CH = 768
QR = ROWS * HL
KP = 224
OUTR = 72
FFL = 704
GU = 2 * FFL
WC = 2176
EPS = 1e-06
TPS = 8
OWN = ROWS // TPS
LOW = -1e30
GAP = 56.0

SP = ("z", "y")
TP = ("x", "c")
F32 = jnp.float32
BF16 = jnp.bfloat16
NT = (((1,), (1,)), ((), ()))


def kernel_pieces(value):
    one = value.astype(BF16).astype(F32)
    rest = value - one
    two = rest.astype(BF16).astype(F32)
    return one, two, rest - two


def payload_kernel(keys, values, gates, out):
    k32 = keys[...].astype(F32)
    norm = jnp.max(jnp.sum(k32 * k32, axis=0, keepdims=True), axis=1, keepdims=True)
    norm = jnp.sqrt(norm) * 1.01
    rows = jnp.concatenate([k32, values[...].astype(F32)], axis=0).T.astype(BF16)
    line = lax.broadcasted_iota(jnp.int32, (16, ROWS), 0)
    side = jnp.concatenate([*kernel_pieces(gates[...]), jnp.ones((HL, ROWS), F32)], axis=0)
    side = jnp.where(line == 15, norm, side)
    left = side[:, 0:128].astype(BF16)
    right = jnp.concatenate([side[:, 128:], jnp.zeros((16, 64), F32)], axis=1).astype(BF16)
    for n in range(YS):
        out[n, 0:ROWS, :] = rows
        out[n, ROWS : ROWS + 16, :] = left
        out[n, ROWS + 16 : KP, :] = right


def payload(keys, values, gates):
    return pl.pallas_call(
        payload_kernel,
        out_shape=jax.ShapeDtypeStruct((YS, KP, 128), BF16),
        cost_estimate=pl.CostEstimate(flops=100_000, bytes_accessed=500_000, transcendentals=0),
        name="payload",
    )(keys, values, gates)


def grid_z(zh, zl):
    z = jnp.int32(0)
    for a in range(ZH):
        for b in range(QG):
            z = jnp.where((zh == a) & (zl == b), ZGRID[a][b], z)
    return z


def attention_kernel(pos, kv0, kv1, q0, q1, q2, q3, o0, o1, o2, o3, kc, vt, qt, acc, ls, ms):
    kv = (kv0, kv1)
    q = (q0, q1, q2, q3)
    out = (o0, o1, o2, o3)
    zh = pos[0]
    zl = pos[1]
    y = pos[2]
    mine = grid_z(zh, zl)
    theirs = grid_z(1 - zh, zl)
    upper = jnp.maximum(mine, theirs)
    low_at = jnp.where(mine < theirs, 0, 1)
    kc[:, 128:256] = jnp.zeros((NB * ROWS, 128), BF16)
    kmax = jnp.zeros((1, 1), F32)
    for b in range(NB):
        base = b * ROWS
        block = kv[b // YS].at[b % YS]
        kc[base : base + ROWS, 0:128] = block[0:ROWS, :]
        left = block[192:208, :].astype(F32)
        right = block[208:224, :].astype(F32)
        kc[base : base + 128, 128:144] = left.T.astype(BF16)
        kc[base + 128 : base + ROWS, 128:144] = right.T[0:64].astype(BF16)
        kmax = jnp.maximum(kmax, left[15:16, 0:1])
    for i in range(NB * ROWS // TILE):
        vt[i] = kc[i * TILE : (i + 1) * TILE, 0:128].T[64:128]
    head = jnp.zeros((16, QR), jnp.int32)
    col = lax.broadcasted_iota(jnp.int32, (16, QR), 1)
    for h in range(1, HL):
        head = head + jnp.where(col >= h * ROWS, 1, 0)
    line = lax.broadcasted_iota(jnp.int32, (16, QR), 0)
    chosen = jnp.where((line < 3 * HL) & (line % HL == head), -1.0, 0.0)
    qmax = jnp.zeros((1, 1), F32)
    left = kv0[y, ROWS : ROWS + 16, :].astype(F32)
    right = kv0[y, ROWS + 16 : KP, :].astype(F32)[:, 0:64]
    owned = jnp.concatenate([left, right], axis=1)
    owned = owned[0:4] + owned[4:8] + owned[8:12]
    owned = jnp.concatenate([owned[h : h + 1] for h in range(HL)], axis=1)
    for j in range(QG):
        asked = grid_z(zh, (zl + QG - j) % QG)
        last = jnp.where(asked > upper, 1 - low_at, low_at)
        ends = [rows[YS - 1, 208:224, :].astype(F32)[:, 63:64] for rows in kv]
        ends = jnp.where(last == 0, ends[0], ends[1])
        turned = q[j][...].astype(F32).T
        turned = jnp.concatenate([turned[h * HD : (h + 1) * HD] for h in range(HL)], axis=1)
        norm = jnp.sqrt(jnp.sum(turned * turned, axis=0, keepdims=True))
        qmax = jnp.maximum(qmax, jnp.max(norm, axis=1, keepdims=True))
        ref = jnp.zeros((1, QR), F32)
        for h in range(HL):
            end = ends[h : h + 1] + ends[4 + h : 5 + h] + ends[8 + h : 9 + h]
            ref = jnp.where(head[0:1] == h, end, ref)
        ref = owned if j == 0 else ref
        one, two, three = kernel_pieces(ref - norm * kmax)
        side = jnp.where(line == 12, one, chosen)
        side = jnp.where(line == 13, two, side)
        side = jnp.where(line == 14, three, side)
        qt[j, 0:HD, :] = turned.astype(BF16)
        qt[j, HD:128, :] = jnp.zeros((128 - HD, QR), BF16)
        qt[j, 128:144, :] = side.astype(BF16)
        qt[j, 144:256, :] = jnp.zeros((112, QR), BF16)
    acc[...] = jnp.zeros(acc.shape, F32)
    ls[...] = jnp.zeros(ls.shape, F32)
    ms[...] = jnp.full(ms.shape, LOW, F32)
    fast = (2.0 * qmax * kmax)[0, 0] <= GAP

    def unit(j, hz, masked, bounded):
        def step(i, none):
            tile = hz * (YS * ROWS // TILE) + i
            kk = kc[pl.ds(pl.multiple_of(tile * TILE, TILE), TILE), :]
            vv = vt[tile]
            for n in range(QR // CH):
                cols = slice(n * CH, (n + 1) * CH)
                s = jnp.dot(kk, qt[j, :, cols], preferred_element_type=F32)
                if masked:
                    col = n * CH + lax.broadcasted_iota(jnp.int32, (TILE, CH), 1)
                    for h in range(1, HL):
                        col = jnp.where(col >= ROWS, col - ROWS, col)
                    row = i * TILE + lax.broadcasted_iota(jnp.int32, (TILE, CH), 0)
                    s = jnp.where(row <= col + y * ROWS, s, LOW)
                if bounded:
                    w = jnp.exp(s)
                    ls[j, :, cols] += jnp.sum(w.reshape(TILE // 8, 8, CH), axis=0)
                    acc[j, :, cols] += jnp.dot(vv, w.astype(BF16), preferred_element_type=F32)
                else:
                    old = ms[j, 0:1, cols]
                    new = jnp.maximum(old, jnp.max(s, axis=0, keepdims=True))
                    shrink = jnp.exp(old - new)
                    w = jnp.exp(s - new)
                    ms[j, :, cols] = jnp.broadcast_to(new, (8, CH))
                    part = jnp.sum(w.reshape(TILE // 8, 8, CH), axis=0)
                    ls[j, :, cols] = ls[j, :, cols] * shrink + part
                    got = jnp.dot(vv, w.astype(BF16), preferred_element_type=F32)
                    acc[j, :, cols] = acc[j, :, cols] * shrink + got
            return none

        lax.fori_loop(0, YS * ROWS // TILE, step, 0)

    def units(bounded):
        def one(u, none):
            j = u // ZH
            hz = u % ZH
            asked = grid_z(zh, (zl + QG - j) % QG)
            edge = u == 0
            whole = asked > jnp.where(hz == 0, mine, theirs)

            @pl.when(whole)
            def _():
                unit(j, hz, False, bounded)

            @pl.when(edge)
            def _():
                unit(j, hz, True, bounded)

            return none

        lax.fori_loop(0, QG * ZH, one, 0)

    @pl.when(fast)
    def _():
        units(True)
        ms[...] = jnp.zeros(ms.shape, F32)

    @pl.when(jnp.logical_not(fast))
    def _():
        units(False)

    spot = lax.broadcasted_iota(jnp.int32, (8, 256), 1)
    pick = jnp.where((spot >= 140) & (spot <= 142), 1.0, 0.0).astype(BF16)
    line = lax.broadcasted_iota(jnp.int32, (8, QR), 0)
    for j in range(QG):
        shift = jnp.dot(pick, qt[j], preferred_element_type=F32)[0:1]
        total = jnp.sum(ls[j], axis=0, keepdims=True)
        top = jnp.where(total > 0.0, ms[j, 0:1, :] - shift, LOW)
        stats = jnp.zeros((8, QR), F32)
        for k, part in enumerate(kernel_pieces(total) + kernel_pieces(top)):
            stats = jnp.where(line == k, part, stats)
        out[j][0:HD, :] = acc[j].astype(BF16)
        out[j][HD:OUTR, :] = stats.astype(BF16)


def attention(pos, *rest):
    vmem = pl.BlockSpec(memory_space=pltpu.VMEM)
    return pl.pallas_call(
        attention_kernel,
        out_shape=[jax.ShapeDtypeStruct((OUTR, QR), BF16)] * QG,
        in_specs=[pl.BlockSpec(memory_space=pltpu.SMEM)] + [vmem] * (QG + 2),
        out_specs=[vmem] * QG,
        scratch_shapes=[
            pltpu.VMEM((NB * ROWS, 256), BF16),
            pltpu.VMEM((NB * ROWS // TILE, HD, TILE), BF16),
            pltpu.VMEM((QG, 256, QR), BF16),
            pltpu.VMEM((QG, HD, QR), F32),
            pltpu.VMEM((QG, 8, QR), F32),
            pltpu.VMEM((QG, 8, QR), F32),
        ],
        compiler_params=pltpu.CompilerParams(vmem_limit_bytes=48 * 1024 * 1024),
        cost_estimate=pl.CostEstimate(flops=12_000_000_000, bytes_accessed=4_000_000, transcendentals=9_000_000),
        name="attention",
    )(pos, *rest)


def by_core(core, rows, mine, theirs, cols):
    low = rows[0 : ROWS // 2].astype(BF16)
    high = rows[ROWS // 2 :].astype(BF16)
    mine[:, cols] = jnp.where(core == 0, low, high)
    theirs[:, cols] = jnp.where(core == 0, high, low)


def merge_kernel(core, p0, p1, p2, p3, gates, weight, mine, theirs):
    parts = (p0, p1, p2, p3)
    tops = []
    sums = []
    for j in range(QG):
        stats = parts[j][HD:OUTR, :].astype(F32)
        sums.append(stats[0:1] + stats[1:2] + stats[2:3])
        tops.append(jnp.where(sums[j] > 0.0, stats[3:4] + stats[4:5] + stats[5:6], LOW))
    top = tops[0]
    for j in range(1, QG):
        top = jnp.maximum(top, tops[j])
    total = jnp.zeros((1, QR), F32)
    mixed = jnp.zeros((HD, QR), F32)
    for j in range(QG):
        scale = jnp.exp(tops[j] - top)
        total = total + sums[j] * scale
        mixed = mixed + parts[j][0:HD, :].astype(F32) * scale
    rows = (mixed / total).T
    rows = jnp.concatenate([rows[h * ROWS : (h + 1) * ROWS] for h in range(HL)], axis=1)
    rows = rows * jax.nn.sigmoid(gates[...].astype(F32))
    order = [x * 2 + c for c in range(2) for x in range(TPS // 2)]
    gated = jnp.concatenate([rows[k * OWN : (k + 1) * OWN] for k in order], axis=0).astype(BF16)
    projected = jnp.dot(gated, weight[...], preferred_element_type=F32)
    by_core(core[0], projected, mine, theirs, slice(None))


def halves(wide):
    return [jax.ShapeDtypeStruct((ROWS // 2, wide), BF16)] * 2


def merge(core, parts, gates, weight):
    vmem = pl.BlockSpec(memory_space=pltpu.VMEM)
    return pl.pallas_call(
        merge_kernel,
        out_shape=halves(weight.shape[1]),
        in_specs=[pl.BlockSpec(memory_space=pltpu.SMEM)] + [vmem] * (QG + 2),
        out_specs=[vmem] * 2,
        compiler_params=pltpu.CompilerParams(vmem_limit_bytes=32 * 1024 * 1024),
        cost_estimate=pl.CostEstimate(flops=400_000_000, bytes_accessed=2_000_000, transcendentals=50_000),
        name="merge",
    )(core, *parts, gates, weight)


FC = 1024
DEEP = 4


def ffn_kernel(core, rows, weights, mine, theirs, wv, acc, hid, sems):
    count = weights.shape[0] // FC

    def first(k):
        at = (pl.ds(k * FC, FC), pl.ds(0, GU))
        return pltpu.make_async_copy(weights.at[at], wv.at[at], sems.at[k])

    def second(k):
        at = (pl.ds(k * FC, FC), pl.ds(GU, WC - GU))
        return pltpu.make_async_copy(weights.at[at], wv.at[at], sems.at[count + k])

    moves = [first(k) for k in range(count)] + [second(k) for k in range(count)]
    for k in range(DEEP):
        moves[k].start()

    def arrive(k):
        moves[k].wait()
        if k + DEEP < len(moves):
            moves[k + DEEP].start()

    for k in range(count):
        arrive(k)
        part = jnp.dot(
            rows[:, k * FC : (k + 1) * FC],
            wv[k * FC : (k + 1) * FC, 0:GU],
            preferred_element_type=F32,
        )
        if k == 0:
            acc[...] = part
        else:
            acc[...] += part
    gate = acc[:, 0:FFL]
    up = acc[:, FFL:GU]
    hidden = gate / (1.0 + jnp.exp(-gate)) * up
    hid[:, FFL:] = jnp.zeros((ROWS, WC - GU - FFL), BF16)
    hid[:, 0:FFL] = hidden.astype(BF16)
    for k in range(count):
        arrive(count + k)
        part = lax.dot_general(
            hid[...], wv[k * FC : (k + 1) * FC, GU:WC], NT, preferred_element_type=F32
        )
        by_core(core[0], part, mine, theirs, slice(k * FC, (k + 1) * FC))


def ffn(core, rows, weights):
    wide = weights.shape[0]
    vmem = pl.BlockSpec(memory_space=pltpu.VMEM)
    return pl.pallas_call(
        ffn_kernel,
        out_shape=halves(wide),
        in_specs=[pl.BlockSpec(memory_space=pltpu.SMEM), vmem, pl.BlockSpec(memory_space=pltpu.HBM)],
        out_specs=[vmem] * 2,
        scratch_shapes=[
            pltpu.VMEM((wide, WC), BF16),
            pltpu.VMEM((ROWS, GU), F32),
            pltpu.VMEM((ROWS, WC - GU), BF16),
            pltpu.SemaphoreType.DMA((2 * (wide // FC),)),
        ],
        compiler_params=pltpu.CompilerParams(vmem_limit_bytes=48 * 1024 * 1024),
        cost_estimate=pl.CostEstimate(flops=1_700_000_000, bytes_accessed=10_000_000, transcendentals=140_000),
        name="ffn",
    )(core, rows, weights)


def copies(value, axis):
    sent = jnp.broadcast_to(value[None], (lax.axis_size(axis), *value.shape))
    return lax.all_to_all(sent, axis, 0, 0, tiled=True)


def sum_at_owner(mine, theirs):
    given = lax.ppermute(theirs, "c", [(0, 1), (1, 0)])
    both = (mine.astype(F32) + given.astype(F32)).astype(BF16)
    blocks = both.reshape(TPS // 2, OWN, both.shape[1])
    arrived = lax.all_to_all(blocks, "x", 0, 0, tiled=True)
    return arrived.astype(F32).sum(axis=0)


def rms_scale(rows, gain):
    mean_sq = jnp.mean(rows * rows, axis=-1, keepdims=True)
    return rows * lax.rsqrt(mean_sq + EPS) * gain


def shards(
    resid,
    queries,
    keys,
    values,
    log_gates,
    out_gate,
    out_weight,
    post_gain,
    pre_gain,
    ffn_gain,
    gate_weight,
    up_weight,
    down_weight,
):
    pairs = [(row, i, (i + r) % QG, r) for row in ZGRID for i in range(QG) for r in range(1, QG)]
    partner = {a: b for column in zip(*ZGRID) for a, b in (column, column[::-1])}
    asks = [(row[i], row[k], r) for row, i, k, r in pairs if row[i] > min(row[k], partner[row[k]])]

    def ask(r):
        return [(q, k) for q, k, turn in asks if turn == r]

    def answer(r):
        return [(k, q) for q, k, turn in asks if turn == r]

    swap = [(partner[d], d) for row in ZGRID for d in row if max(row) > partner[d]]
    pad = jnp.zeros((gate_weight.shape[0], WC - GU - FFL), BF16)
    packed = jnp.concatenate([gate_weight, up_weight, down_weight.T, pad], axis=1)
    weights = lax.all_gather(packed, SP, axis=0, tiled=True)
    scaled = queries * jnp.asarray(HD**-0.5, BF16)
    q_all = [scaled] + [lax.ppermute(scaled, "z", ask(r)) for r in range(1, QG)]
    held = lax.all_to_all(payload(keys.T, values.T, log_gates.T), "y", 0, 0, tiled=True)
    lent = lax.ppermute(held, "z", swap)
    z = lax.axis_index("z")
    zh = sum(jnp.where(z == ZGRID[a][b], a, 0) for a in range(ZH) for b in range(QG))
    zl = sum(jnp.where(z == ZGRID[a][b], b, 0) for a in range(ZH) for b in range(QG))
    pos = jnp.stack([zh, zl, lax.axis_index("y")]).astype(jnp.int32)
    parts = attention(pos, held, lent, *q_all)
    parts = [parts[0]] + [lax.ppermute(parts[r], "z", answer(r)) for r in range(1, QG)]
    core = lax.axis_index("c").astype(jnp.int32)[None]
    projected = sum_at_owner(*merge(core, parts, out_gate, out_weight))
    mixed = resid.astype(F32) + rms_scale(projected, post_gain)
    normed = rms_scale(mixed, pre_gain).astype(BF16)
    along = copies(normed, "x").reshape(ROWS // 2, -1)
    normed_all = lax.all_gather(along, "c", axis=0, tiled=True)
    total = sum_at_owner(*ffn(core, normed_all, weights))
    return (mixed + rms_scale(total, ffn_gain)).astype(BF16)


def solution(mesh):
    split = Mesh(mesh.devices.reshape(8, YS, 4, 2), ("z", "y", "x", "c"))
    in_specs = (
        P((*SP, *TP), None),
        P(SP, TP),
        P(SP, TP),
        P(SP, TP),
        P(SP, TP),
        P(SP, TP),
        P(TP, None),
        P(),
        P(),
        P(),
        P(SP, TP),
        P(SP, TP),
        P(TP, SP),
    )
    return jax.shard_map(
        shards, mesh=split, in_specs=in_specs, out_specs=P((*SP, *TP), None), check_vma=False
    )
```

```python
import jax
import jax.numpy as jnp
from jax import lax
from jax.experimental import pallas as pl
from jax.experimental.pallas import tpu as pltpu
from jax.sharding import Mesh
from jax.sharding import PartitionSpec as P

HD = 64
HL = 4
ROWS = 192
QG = 4
ZH = 8 // QG
ZGRID = ((0, 2, 4, 6), (7, 1, 3, 5))
YS = 8
NB = ZH * YS
TILE = 1536
CH = 768
QR = ROWS * HL
KP = 224
OUTR = 72
FFL = 704
GU = 2 * FFL
WC = 2176
EPS = 1e-06
TPS = 8
OWN = ROWS // TPS
LOW = -1e30
GAP = 56.0

SP = ("z", "y")
TP = ("x", "c")
F32 = jnp.float32
BF16 = jnp.bfloat16
NT = (((1,), (1,)), ((), ()))


def kernel_pieces(value):
    one = value.astype(BF16).astype(F32)
    rest = value - one
    two = rest.astype(BF16).astype(F32)
    return one, two, rest - two


def payload_kernel(keys, values, gates, out):
    k32 = keys[...].astype(F32)
    norm = jnp.max(jnp.sum(k32 * k32, axis=0, keepdims=True), axis=1, keepdims=True)
    norm = jnp.sqrt(norm) * 1.01
    rows = jnp.concatenate([k32, values[...].astype(F32)], axis=0).T.astype(BF16)
    line = lax.broadcasted_iota(jnp.int32, (16, ROWS), 0)
    side = jnp.concatenate([*kernel_pieces(gates[...]), jnp.ones((HL, ROWS), F32)], axis=0)
    side = jnp.where(line == 15, norm, side)
    left = side[:, 0:128].astype(BF16)
    right = jnp.concatenate([side[:, 128:], jnp.zeros((16, 64), F32)], axis=1).astype(BF16)
    out[0:ROWS, :] = rows
    out[ROWS : ROWS + 16, :] = left
    out[ROWS + 16 : KP, :] = right


def payload(keys, values, gates):
    return pl.pallas_call(
        payload_kernel,
        out_shape=jax.ShapeDtypeStruct((KP, 128), BF16),
        cost_estimate=pl.CostEstimate(flops=100_000, bytes_accessed=500_000, transcendentals=0),
        name="payload",
    )(keys, values, gates)


def grid_z(zh, zl):
    z = jnp.int32(0)
    for a in range(ZH):
        for b in range(QG):
            z = jnp.where((zh == a) & (zl == b), ZGRID[a][b], z)
    return z


def attention_kernel(pos, kv0, kv1, q0, q1, q2, q3, o0, o1, o2, o3, kc, vt, qt, acc, ls, ms):
    kv = (kv0, kv1)
    q = (q0, q1, q2, q3)
    out = (o0, o1, o2, o3)
    zh = pos[0]
    zl = pos[1]
    y = pos[2]
    mine = grid_z(zh, zl)
    theirs = grid_z(1 - zh, zl)
    upper = jnp.maximum(mine, theirs)
    low_at = jnp.where(mine < theirs, 0, 1)
    kc[:, 128:256] = jnp.zeros((NB * ROWS, 128), BF16)
    kmax = jnp.zeros((1, 1), F32)
    for b in range(NB):
        base = b * ROWS
        block = kv[b // YS].at[b % YS]
        kc[base : base + ROWS, 0:128] = block[0:ROWS, :]
        left = block[192:208, :].astype(F32)
        right = block[208:224, :].astype(F32)
        kc[base : base + 128, 128:144] = left.T.astype(BF16)
        kc[base + 128 : base + ROWS, 128:144] = right.T[0:64].astype(BF16)
        kmax = jnp.maximum(kmax, left[15:16, 0:1])
    for i in range(NB * ROWS // TILE):
        vt[i] = kc[i * TILE : (i + 1) * TILE, 0:128].T[64:128]
    head = jnp.zeros((16, QR), jnp.int32)
    col = lax.broadcasted_iota(jnp.int32, (16, QR), 1)
    for h in range(1, HL):
        head = head + jnp.where(col >= h * ROWS, 1, 0)
    line = lax.broadcasted_iota(jnp.int32, (16, QR), 0)
    chosen = jnp.where((line < 3 * HL) & (line % HL == head), -1.0, 0.0)
    qmax = jnp.zeros((1, 1), F32)
    left = kv0[y, ROWS : ROWS + 16, :].astype(F32)
    right = kv0[y, ROWS + 16 : KP, :].astype(F32)[:, 0:64]
    owned = jnp.concatenate([left, right], axis=1)
    owned = owned[0:4] + owned[4:8] + owned[8:12]
    owned = jnp.concatenate([owned[h : h + 1] for h in range(HL)], axis=1)
    for j in range(QG):
        asked = grid_z(zh, (zl + QG - j) % QG)
        last = jnp.where(asked > upper, 1 - low_at, low_at)
        ends = [rows[YS - 1, 208:224, :].astype(F32)[:, 63:64] for rows in kv]
        ends = jnp.where(last == 0, ends[0], ends[1])
        turned = q[j][...].astype(F32).T
        turned = jnp.concatenate([turned[h * HD : (h + 1) * HD] for h in range(HL)], axis=1)
        norm = jnp.sqrt(jnp.sum(turned * turned, axis=0, keepdims=True))
        qmax = jnp.maximum(qmax, jnp.max(norm, axis=1, keepdims=True))
        ref = jnp.zeros((1, QR), F32)
        for h in range(HL):
            end = ends[h : h + 1] + ends[4 + h : 5 + h] + ends[8 + h : 9 + h]
            ref = jnp.where(head[0:1] == h, end, ref)
        ref = owned if j == 0 else ref
        one, two, three = kernel_pieces(ref - norm * kmax)
        side = jnp.where(line == 12, one, chosen)
        side = jnp.where(line == 13, two, side)
        side = jnp.where(line == 14, three, side)
        qt[j, 0:HD, :] = turned.astype(BF16)
        qt[j, HD:128, :] = jnp.zeros((128 - HD, QR), BF16)
        qt[j, 128:144, :] = side.astype(BF16)
        qt[j, 144:256, :] = jnp.zeros((112, QR), BF16)
    acc[...] = jnp.zeros(acc.shape, F32)
    ls[...] = jnp.zeros(ls.shape, F32)
    ms[...] = jnp.full(ms.shape, LOW, F32)
    fast = (2.0 * qmax * kmax)[0, 0] <= GAP

    def unit(j, hz, masked, bounded):
        def step(i, none):
            tile = hz * (YS * ROWS // TILE) + i
            kk = kc[pl.ds(pl.multiple_of(tile * TILE, TILE), TILE), :]
            vv = vt[tile]
            for n in range(QR // CH):
                cols = slice(n * CH, (n + 1) * CH)
                s = jnp.dot(kk, qt[j, :, cols], preferred_element_type=F32)
                if masked:
                    col = n * CH + lax.broadcasted_iota(jnp.int32, (TILE, CH), 1)
                    for h in range(1, HL):
                        col = jnp.where(col >= ROWS, col - ROWS, col)
                    row = i * TILE + lax.broadcasted_iota(jnp.int32, (TILE, CH), 0)
                    s = jnp.where(row <= col + y * ROWS, s, LOW)
                if bounded:
                    w = jnp.exp(s)
                    ls[j, :, cols] += jnp.sum(w.reshape(TILE // 8, 8, CH), axis=0)
                    acc[j, :, cols] += jnp.dot(vv, w.astype(BF16), preferred_element_type=F32)
                else:
                    old = ms[j, 0:1, cols]
                    new = jnp.maximum(old, jnp.max(s, axis=0, keepdims=True))
                    shrink = jnp.exp(old - new)
                    w = jnp.exp(s - new)
                    ms[j, :, cols] = jnp.broadcast_to(new, (8, CH))
                    part = jnp.sum(w.reshape(TILE // 8, 8, CH), axis=0)
                    ls[j, :, cols] = ls[j, :, cols] * shrink + part
                    got = jnp.dot(vv, w.astype(BF16), preferred_element_type=F32)
                    acc[j, :, cols] = acc[j, :, cols] * shrink + got
            return none

        lax.fori_loop(0, YS * ROWS // TILE, step, 0)

    def units(bounded):
        def one(u, none):
            j = u // ZH
            hz = u % ZH
            asked = grid_z(zh, (zl + QG - j) % QG)
            edge = u == 0
            whole = asked > jnp.where(hz == 0, mine, theirs)

            @pl.when(whole)
            def _():
                unit(j, hz, False, bounded)

            @pl.when(edge)
            def _():
                unit(j, hz, True, bounded)

            return none

        lax.fori_loop(0, QG * ZH, one, 0)

    @pl.when(fast)
    def _():
        units(True)
        ms[...] = jnp.zeros(ms.shape, F32)

    @pl.when(jnp.logical_not(fast))
    def _():
        units(False)

    spot = lax.broadcasted_iota(jnp.int32, (8, 256), 1)
    pick = jnp.where((spot >= 140) & (spot <= 142), 1.0, 0.0).astype(BF16)
    line = lax.broadcasted_iota(jnp.int32, (8, QR), 0)
    for j in range(QG):
        shift = jnp.dot(pick, qt[j], preferred_element_type=F32)[0:1]
        total = jnp.sum(ls[j], axis=0, keepdims=True)
        top = jnp.where(total > 0.0, ms[j, 0:1, :] - shift, LOW)
        stats = jnp.zeros((8, QR), F32)
        for k, part in enumerate(kernel_pieces(total) + kernel_pieces(top)):
            stats = jnp.where(line == k, part, stats)
        out[j][0:HD, :] = acc[j].astype(BF16)
        out[j][HD:OUTR, :] = stats.astype(BF16)


def attention(pos, *rest):
    vmem = pl.BlockSpec(memory_space=pltpu.VMEM)
    return pl.pallas_call(
        attention_kernel,
        out_shape=[jax.ShapeDtypeStruct((OUTR, QR), BF16)] * QG,
        in_specs=[pl.BlockSpec(memory_space=pltpu.SMEM)] + [vmem] * (QG + 2),
        out_specs=[vmem] * QG,
        scratch_shapes=[
            pltpu.VMEM((NB * ROWS, 256), BF16),
            pltpu.VMEM((NB * ROWS // TILE, HD, TILE), BF16),
            pltpu.VMEM((QG, 256, QR), BF16),
            pltpu.VMEM((QG, HD, QR), F32),
            pltpu.VMEM((QG, 8, QR), F32),
            pltpu.VMEM((QG, 8, QR), F32),
        ],
        compiler_params=pltpu.CompilerParams(vmem_limit_bytes=48 * 1024 * 1024),
        cost_estimate=pl.CostEstimate(flops=12_000_000_000, bytes_accessed=4_000_000, transcendentals=9_000_000),
        name="attention",
    )(pos, *rest)


def by_core(core, rows, mine, theirs, cols):
    low = rows[0 : ROWS // 2].astype(BF16)
    high = rows[ROWS // 2 :].astype(BF16)
    mine[:, cols] = jnp.where(core == 0, low, high)
    theirs[:, cols] = jnp.where(core == 0, high, low)


def merge_kernel(core, p0, p1, p2, p3, gates, weight, mine, theirs):
    parts = (p0, p1, p2, p3)
    tops = []
    sums = []
    for j in range(QG):
        stats = parts[j][HD:OUTR, :].astype(F32)
        sums.append(stats[0:1] + stats[1:2] + stats[2:3])
        tops.append(jnp.where(sums[j] > 0.0, stats[3:4] + stats[4:5] + stats[5:6], LOW))
    top = tops[0]
    for j in range(1, QG):
        top = jnp.maximum(top, tops[j])
    total = jnp.zeros((1, QR), F32)
    mixed = jnp.zeros((HD, QR), F32)
    for j in range(QG):
        scale = jnp.exp(tops[j] - top)
        total = total + sums[j] * scale
        mixed = mixed + parts[j][0:HD, :].astype(F32) * scale
    rows = (mixed / total).T
    rows = jnp.concatenate([rows[h * ROWS : (h + 1) * ROWS] for h in range(HL)], axis=1)
    rows = rows * jax.nn.sigmoid(gates[...].astype(F32))
    order = [x * 2 + c for c in range(2) for x in range(TPS // 2)]
    gated = jnp.concatenate([rows[k * OWN : (k + 1) * OWN] for k in order], axis=0).astype(BF16)
    projected = jnp.dot(gated, weight[...], preferred_element_type=F32)
    by_core(core[0], projected, mine, theirs, slice(None))


def halves(wide):
    return [jax.ShapeDtypeStruct((ROWS // 2, wide), BF16)] * 2


def merge(core, parts, gates, weight):
    vmem = pl.BlockSpec(memory_space=pltpu.VMEM)
    return pl.pallas_call(
        merge_kernel,
        out_shape=halves(weight.shape[1]),
        in_specs=[pl.BlockSpec(memory_space=pltpu.SMEM)] + [vmem] * (QG + 2),
        out_specs=[vmem] * 2,
        compiler_params=pltpu.CompilerParams(vmem_limit_bytes=32 * 1024 * 1024),
        cost_estimate=pl.CostEstimate(flops=400_000_000, bytes_accessed=2_000_000, transcendentals=50_000),
        name="merge",
    )(core, *parts, gates, weight)


FC = 1024
DEEP = 4


def ffn_kernel(core, rows, weights, mine, theirs, wv, acc, hid, sems):
    count = weights.shape[0] // FC

    def first(k):
        at = (pl.ds(k * FC, FC), pl.ds(0, GU))
        return pltpu.make_async_copy(weights.at[at], wv.at[at], sems.at[k])

    def second(k):
        at = (pl.ds(k * FC, FC), pl.ds(GU, WC - GU))
        return pltpu.make_async_copy(weights.at[at], wv.at[at], sems.at[count + k])

    moves = [first(k) for k in range(count)] + [second(k) for k in range(count)]
    for k in range(DEEP):
        moves[k].start()

    def arrive(k):
        moves[k].wait()
        if k + DEEP < len(moves):
            moves[k + DEEP].start()

    for k in range(count):
        arrive(k)
        part = jnp.dot(
            rows[:, k * FC : (k + 1) * FC],
            wv[k * FC : (k + 1) * FC, 0:GU],
            preferred_element_type=F32,
        )
        if k == 0:
            acc[...] = part
        else:
            acc[...] += part
    gate = acc[:, 0:FFL]
    up = acc[:, FFL:GU]
    hidden = gate / (1.0 + jnp.exp(-gate)) * up
    hid[:, FFL:] = jnp.zeros((ROWS, WC - GU - FFL), BF16)
    hid[:, 0:FFL] = hidden.astype(BF16)
    for k in range(count):
        arrive(count + k)
        part = lax.dot_general(
            hid[...], wv[k * FC : (k + 1) * FC, GU:WC], NT, preferred_element_type=F32
        )
        by_core(core[0], part, mine, theirs, slice(k * FC, (k + 1) * FC))


def ffn(core, rows, weights):
    wide = weights.shape[0]
    vmem = pl.BlockSpec(memory_space=pltpu.VMEM)
    return pl.pallas_call(
        ffn_kernel,
        out_shape=halves(wide),
        in_specs=[pl.BlockSpec(memory_space=pltpu.SMEM), vmem, pl.BlockSpec(memory_space=pltpu.HBM)],
        out_specs=[vmem] * 2,
        scratch_shapes=[
            pltpu.VMEM((wide, WC), BF16),
            pltpu.VMEM((ROWS, GU), F32),
            pltpu.VMEM((ROWS, WC - GU), BF16),
            pltpu.SemaphoreType.DMA((2 * (wide // FC),)),
        ],
        compiler_params=pltpu.CompilerParams(vmem_limit_bytes=48 * 1024 * 1024),
        cost_estimate=pl.CostEstimate(flops=1_700_000_000, bytes_accessed=10_000_000, transcendentals=140_000),
        name="ffn",
    )(core, rows, weights)


def copies(value, axis):
    sent = jnp.broadcast_to(value[None], (lax.axis_size(axis), *value.shape))
    return lax.all_to_all(sent, axis, 0, 0, tiled=True)


def sum_at_owner(mine, theirs):
    given = lax.ppermute(theirs, "c", [(0, 1), (1, 0)])
    both = (mine.astype(F32) + given.astype(F32)).astype(BF16)
    blocks = both.reshape(TPS // 2, OWN, both.shape[1])
    arrived = lax.all_to_all(blocks, "x", 0, 0, tiled=True)
    return arrived.astype(F32).sum(axis=0)


def rms_scale(rows, gain):
    mean_sq = jnp.mean(rows * rows, axis=-1, keepdims=True)
    return rows * lax.rsqrt(mean_sq + EPS) * gain


def shards(
    resid,
    queries,
    keys,
    values,
    log_gates,
    out_gate,
    out_weight,
    post_gain,
    pre_gain,
    ffn_gain,
    gate_weight,
    up_weight,
    down_weight,
):
    pairs = [(row, i, (i + r) % QG, r) for row in ZGRID for i in range(QG) for r in range(1, QG)]
    partner = {a: b for column in zip(*ZGRID) for a, b in (column, column[::-1])}
    asks = [(row[i], row[k], r) for row, i, k, r in pairs if row[i] > min(row[k], partner[row[k]])]

    def ask(r):
        return [(q, k) for q, k, turn in asks if turn == r]

    def answer(r):
        return [(k, q) for q, k, turn in asks if turn == r]

    swap = [(partner[d], d) for row in ZGRID for d in row if max(row) > partner[d]]
    pad = jnp.zeros((gate_weight.shape[0], WC - GU - FFL), BF16)
    packed = jnp.concatenate([gate_weight, up_weight, down_weight.T, pad], axis=1)
    weights = lax.all_gather(packed, SP, axis=0, tiled=True)
    scaled = queries * jnp.asarray(HD**-0.5, BF16)
    q_all = [scaled] + [lax.ppermute(scaled, "z", ask(r)) for r in range(1, QG)]
    held = lax.all_gather(payload(keys.T, values.T, log_gates.T), "y")
    lent = lax.ppermute(held, "z", swap)
    z = lax.axis_index("z")
    zh = sum(jnp.where(z == ZGRID[a][b], a, 0) for a in range(ZH) for b in range(QG))
    zl = sum(jnp.where(z == ZGRID[a][b], b, 0) for a in range(ZH) for b in range(QG))
    pos = jnp.stack([zh, zl, lax.axis_index("y")]).astype(jnp.int32)
    parts = attention(pos, held, lent, *q_all)
    parts = [parts[0]] + [lax.ppermute(parts[r], "z", answer(r)) for r in range(1, QG)]
    core = lax.axis_index("c").astype(jnp.int32)[None]
    projected = sum_at_owner(*merge(core, parts, out_gate, out_weight))
    mixed = resid.astype(F32) + rms_scale(projected, post_gain)
    normed = rms_scale(mixed, pre_gain).astype(BF16)
    along = copies(normed, "x").reshape(ROWS // 2, -1)
    normed_all = lax.all_gather(along, "c", axis=0, tiled=True)
    total = sum_at_owner(*ffn(core, normed_all, weights))
    return (mixed + rms_scale(total, ffn_gain)).astype(BF16)


def solution(mesh):
    split = Mesh(mesh.devices.reshape(8, YS, 4, 2), ("z", "y", "x", "c"))
    in_specs = (
        P((*SP, *TP), None),
        P(SP, TP),
        P(SP, TP),
        P(SP, TP),
        P(SP, TP),
        P(SP, TP),
        P(TP, None),
        P(),
        P(),
        P(),
        P(SP, TP),
        P(SP, TP),
        P(TP, SP),
    )
    return jax.shard_map(
        shards, mesh=split, in_specs=in_specs, out_specs=P((*SP, *TP), None), check_vma=False
    )
```

```python
import jax
import jax.numpy as jnp
from jax import lax
from jax.experimental import pallas as pl
from jax.experimental.pallas import tpu as pltpu
from jax.sharding import Mesh
from jax.sharding import PartitionSpec as P

HD = 64
HL = 4
ROWS = 192
QG = 4
ZH = 8 // QG
ZGRID = ((0, 2, 5, 7), (1, 3, 4, 6))
YS = 8
NB = ZH * YS
TILE = 1536
CH = 768
QR = ROWS * HL
KP = 224
OUTR = 72
FFL = 704
GU = 2 * FFL
WC = 2176
EPS = 1e-06
TPS = 8
OWN = ROWS // TPS
LOW = -1e30
GAP = 56.0

SP = ("z", "y")
TP = ("x", "c")
F32 = jnp.float32
BF16 = jnp.bfloat16
NT = (((1,), (1,)), ((), ()))


def kernel_pieces(value):
    one = value.astype(BF16).astype(F32)
    rest = value - one
    two = rest.astype(BF16).astype(F32)
    return one, two, rest - two


def payload_kernel(keys, values, gates, out):
    k32 = keys[...].astype(F32)
    norm = jnp.max(jnp.sum(k32 * k32, axis=0, keepdims=True), axis=1, keepdims=True)
    norm = jnp.sqrt(norm) * 1.01
    rows = jnp.concatenate([k32, values[...].astype(F32)], axis=0).T.astype(BF16)
    line = lax.broadcasted_iota(jnp.int32, (16, ROWS), 0)
    side = jnp.concatenate([*kernel_pieces(gates[...]), jnp.ones((HL, ROWS), F32)], axis=0)
    side = jnp.where(line == 15, norm, side)
    left = side[:, 0:128].astype(BF16)
    right = jnp.concatenate([side[:, 128:], jnp.zeros((16, 64), F32)], axis=1).astype(BF16)
    out[0:ROWS, :] = rows
    out[ROWS : ROWS + 16, :] = left
    out[ROWS + 16 : KP, :] = right


def payload(keys, values, gates):
    return pl.pallas_call(
        payload_kernel,
        out_shape=jax.ShapeDtypeStruct((KP, 128), BF16),
        cost_estimate=pl.CostEstimate(flops=100_000, bytes_accessed=500_000, transcendentals=0),
        name="payload",
    )(keys, values, gates)


def grid_z(zh, zl):
    z = jnp.int32(0)
    for a in range(ZH):
        for b in range(QG):
            z = jnp.where((zh == a) & (zl == b), ZGRID[a][b], z)
    return z


def attention_kernel(pos, kv0, kv1, q0, q1, q2, q3, o0, o1, o2, o3, kc, vt, qt, acc, ls, ms):
    kv = (kv0, kv1)
    q = (q0, q1, q2, q3)
    out = (o0, o1, o2, o3)
    zh = pos[0]
    zl = pos[1]
    y = pos[2]
    mine = grid_z(zh, zl)
    theirs = grid_z(1 - zh, zl)
    upper = jnp.maximum(mine, theirs)
    low_at = jnp.where(mine < theirs, 0, 1)
    kc[:, 128:256] = jnp.zeros((NB * ROWS, 128), BF16)
    kmax = jnp.zeros((1, 1), F32)
    for b in range(NB):
        base = b * ROWS
        block = kv[b // YS].at[b % YS]
        kc[base : base + ROWS, 0:128] = block[0:ROWS, :]
        left = block[192:208, :].astype(F32)
        right = block[208:224, :].astype(F32)
        kc[base : base + 128, 128:144] = left.T.astype(BF16)
        kc[base + 128 : base + ROWS, 128:144] = right.T[0:64].astype(BF16)
        kmax = jnp.maximum(kmax, left[15:16, 0:1])
    for i in range(NB * ROWS // TILE):
        vt[i] = kc[i * TILE : (i + 1) * TILE, 0:128].T[64:128]
    head = jnp.zeros((16, QR), jnp.int32)
    col = lax.broadcasted_iota(jnp.int32, (16, QR), 1)
    for h in range(1, HL):
        head = head + jnp.where(col >= h * ROWS, 1, 0)
    line = lax.broadcasted_iota(jnp.int32, (16, QR), 0)
    chosen = jnp.where((line < 3 * HL) & (line % HL == head), -1.0, 0.0)
    qmax = jnp.zeros((1, 1), F32)
    left = kv0[y, ROWS : ROWS + 16, :].astype(F32)
    right = kv0[y, ROWS + 16 : KP, :].astype(F32)[:, 0:64]
    owned = jnp.concatenate([left, right], axis=1)
    owned = owned[0:4] + owned[4:8] + owned[8:12]
    owned = jnp.concatenate([owned[h : h + 1] for h in range(HL)], axis=1)
    for j in range(QG):
        asked = grid_z(zh, (zl + QG - j) % QG)
        last = jnp.where(asked > upper, 1 - low_at, low_at)
        ends = [rows[YS - 1, 208:224, :].astype(F32)[:, 63:64] for rows in kv]
        ends = jnp.where(last == 0, ends[0], ends[1])
        turned = q[j][...].astype(F32).T
        turned = jnp.concatenate([turned[h * HD : (h + 1) * HD] for h in range(HL)], axis=1)
        norm = jnp.sqrt(jnp.sum(turned * turned, axis=0, keepdims=True))
        qmax = jnp.maximum(qmax, jnp.max(norm, axis=1, keepdims=True))
        ref = jnp.zeros((1, QR), F32)
        for h in range(HL):
            end = ends[h : h + 1] + ends[4 + h : 5 + h] + ends[8 + h : 9 + h]
            ref = jnp.where(head[0:1] == h, end, ref)
        ref = owned if j == 0 else ref
        one, two, three = kernel_pieces(ref - norm * kmax)
        side = jnp.where(line == 12, one, chosen)
        side = jnp.where(line == 13, two, side)
        side = jnp.where(line == 14, three, side)
        qt[j, 0:HD, :] = turned.astype(BF16)
        qt[j, HD:128, :] = jnp.zeros((128 - HD, QR), BF16)
        qt[j, 128:144, :] = side.astype(BF16)
        qt[j, 144:256, :] = jnp.zeros((112, QR), BF16)
    acc[...] = jnp.zeros(acc.shape, F32)
    ls[...] = jnp.zeros(ls.shape, F32)
    ms[...] = jnp.full(ms.shape, LOW, F32)
    fast = (2.0 * qmax * kmax)[0, 0] <= GAP

    def unit(j, hz, masked, bounded):
        def step(i, none):
            tile = hz * (YS * ROWS // TILE) + i
            kk = kc[pl.ds(pl.multiple_of(tile * TILE, TILE), TILE), :]
            vv = vt[tile]
            for n in range(QR // CH):
                cols = slice(n * CH, (n + 1) * CH)
                s = jnp.dot(kk, qt[j, :, cols], preferred_element_type=F32)
                if masked:
                    col = n * CH + lax.broadcasted_iota(jnp.int32, (TILE, CH), 1)
                    for h in range(1, HL):
                        col = jnp.where(col >= ROWS, col - ROWS, col)
                    row = i * TILE + lax.broadcasted_iota(jnp.int32, (TILE, CH), 0)
                    s = jnp.where(row <= col + y * ROWS, s, LOW)
                if bounded:
                    w = jnp.exp(s)
                    ls[j, :, cols] += jnp.sum(w.reshape(TILE // 8, 8, CH), axis=0)
                    acc[j, :, cols] += jnp.dot(vv, w.astype(BF16), preferred_element_type=F32)
                else:
                    old = ms[j, 0:1, cols]
                    new = jnp.maximum(old, jnp.max(s, axis=0, keepdims=True))
                    shrink = jnp.exp(old - new)
                    w = jnp.exp(s - new)
                    ms[j, :, cols] = jnp.broadcast_to(new, (8, CH))
                    part = jnp.sum(w.reshape(TILE // 8, 8, CH), axis=0)
                    ls[j, :, cols] = ls[j, :, cols] * shrink + part
                    got = jnp.dot(vv, w.astype(BF16), preferred_element_type=F32)
                    acc[j, :, cols] = acc[j, :, cols] * shrink + got
            return none

        lax.fori_loop(0, YS * ROWS // TILE, step, 0)

    def units(bounded):
        def one(u, none):
            j = u // ZH
            hz = u % ZH
            asked = grid_z(zh, (zl + QG - j) % QG)
            edge = u == 0
            whole = asked > jnp.where(hz == 0, mine, theirs)

            @pl.when(whole)
            def _():
                unit(j, hz, False, bounded)

            @pl.when(edge)
            def _():
                unit(j, hz, True, bounded)

            return none

        lax.fori_loop(0, QG * ZH, one, 0)

    @pl.when(fast)
    def _():
        units(True)
        ms[...] = jnp.zeros(ms.shape, F32)

    @pl.when(jnp.logical_not(fast))
    def _():
        units(False)

    spot = lax.broadcasted_iota(jnp.int32, (8, 256), 1)
    pick = jnp.where((spot >= 140) & (spot <= 142), 1.0, 0.0).astype(BF16)
    line = lax.broadcasted_iota(jnp.int32, (8, QR), 0)
    for j in range(QG):
        shift = jnp.dot(pick, qt[j], preferred_element_type=F32)[0:1]
        total = jnp.sum(ls[j], axis=0, keepdims=True)
        top = jnp.where(total > 0.0, ms[j, 0:1, :] - shift, LOW)
        stats = jnp.zeros((8, QR), F32)
        for k, part in enumerate(kernel_pieces(total) + kernel_pieces(top)):
            stats = jnp.where(line == k, part, stats)
        out[j][0:HD, :] = acc[j].astype(BF16)
        out[j][HD:OUTR, :] = stats.astype(BF16)


def attention(pos, *rest):
    vmem = pl.BlockSpec(memory_space=pltpu.VMEM)
    return pl.pallas_call(
        attention_kernel,
        out_shape=[jax.ShapeDtypeStruct((OUTR, QR), BF16)] * QG,
        in_specs=[pl.BlockSpec(memory_space=pltpu.SMEM)] + [vmem] * (QG + 2),
        out_specs=[vmem] * QG,
        scratch_shapes=[
            pltpu.VMEM((NB * ROWS, 256), BF16),
            pltpu.VMEM((NB * ROWS // TILE, HD, TILE), BF16),
            pltpu.VMEM((QG, 256, QR), BF16),
            pltpu.VMEM((QG, HD, QR), F32),
            pltpu.VMEM((QG, 8, QR), F32),
            pltpu.VMEM((QG, 8, QR), F32),
        ],
        compiler_params=pltpu.CompilerParams(vmem_limit_bytes=48 * 1024 * 1024),
        cost_estimate=pl.CostEstimate(flops=12_000_000_000, bytes_accessed=4_000_000, transcendentals=9_000_000),
        name="attention",
    )(pos, *rest)


def by_core(core, rows, mine, theirs, cols):
    low = rows[0 : ROWS // 2].astype(BF16)
    high = rows[ROWS // 2 :].astype(BF16)
    mine[:, cols] = jnp.where(core == 0, low, high)
    theirs[:, cols] = jnp.where(core == 0, high, low)


def merge_kernel(core, p0, p1, p2, p3, gates, weight, mine, theirs):
    parts = (p0, p1, p2, p3)
    tops = []
    sums = []
    for j in range(QG):
        stats = parts[j][HD:OUTR, :].astype(F32)
        sums.append(stats[0:1] + stats[1:2] + stats[2:3])
        tops.append(jnp.where(sums[j] > 0.0, stats[3:4] + stats[4:5] + stats[5:6], LOW))
    top = tops[0]
    for j in range(1, QG):
        top = jnp.maximum(top, tops[j])
    total = jnp.zeros((1, QR), F32)
    mixed = jnp.zeros((HD, QR), F32)
    for j in range(QG):
        scale = jnp.exp(tops[j] - top)
        total = total + sums[j] * scale
        mixed = mixed + parts[j][0:HD, :].astype(F32) * scale
    rows = (mixed / total).T
    rows = jnp.concatenate([rows[h * ROWS : (h + 1) * ROWS] for h in range(HL)], axis=1)
    rows = rows * jax.nn.sigmoid(gates[...].astype(F32))
    order = [x * 2 + c for c in range(2) for x in range(TPS // 2)]
    gated = jnp.concatenate([rows[k * OWN : (k + 1) * OWN] for k in order], axis=0).astype(BF16)
    projected = jnp.dot(gated, weight[...], preferred_element_type=F32)
    by_core(core[0], projected, mine, theirs, slice(None))


def halves(wide):
    return [jax.ShapeDtypeStruct((ROWS // 2, wide), BF16)] * 2


def merge(core, parts, gates, weight):
    vmem = pl.BlockSpec(memory_space=pltpu.VMEM)
    return pl.pallas_call(
        merge_kernel,
        out_shape=halves(weight.shape[1]),
        in_specs=[pl.BlockSpec(memory_space=pltpu.SMEM)] + [vmem] * (QG + 2),
        out_specs=[vmem] * 2,
        compiler_params=pltpu.CompilerParams(vmem_limit_bytes=32 * 1024 * 1024),
        cost_estimate=pl.CostEstimate(flops=400_000_000, bytes_accessed=2_000_000, transcendentals=50_000),
        name="merge",
    )(core, *parts, gates, weight)


FC = 1024
DEEP = 4


def ffn_kernel(core, rows, weights, mine, theirs, wv, acc, hid, sems):
    count = weights.shape[0] // FC

    def first(k):
        at = (pl.ds(k * FC, FC), pl.ds(0, GU))
        return pltpu.make_async_copy(weights.at[at], wv.at[at], sems.at[k])

    def second(k):
        at = (pl.ds(k * FC, FC), pl.ds(GU, WC - GU))
        return pltpu.make_async_copy(weights.at[at], wv.at[at], sems.at[count + k])

    moves = [first(k) for k in range(count)] + [second(k) for k in range(count)]
    for k in range(DEEP):
        moves[k].start()

    def arrive(k):
        moves[k].wait()
        if k + DEEP < len(moves):
            moves[k + DEEP].start()

    for k in range(count):
        arrive(k)
        part = jnp.dot(
            rows[:, k * FC : (k + 1) * FC],
            wv[k * FC : (k + 1) * FC, 0:GU],
            preferred_element_type=F32,
        )
        if k == 0:
            acc[...] = part
        else:
            acc[...] += part
    gate = acc[:, 0:FFL]
    up = acc[:, FFL:GU]
    hidden = gate / (1.0 + jnp.exp(-gate)) * up
    hid[:, FFL:] = jnp.zeros((ROWS, WC - GU - FFL), BF16)
    hid[:, 0:FFL] = hidden.astype(BF16)
    for k in range(count):
        arrive(count + k)
        part = lax.dot_general(
            hid[...], wv[k * FC : (k + 1) * FC, GU:WC], NT, preferred_element_type=F32
        )
        by_core(core[0], part, mine, theirs, slice(k * FC, (k + 1) * FC))


def ffn(core, rows, weights):
    wide = weights.shape[0]
    vmem = pl.BlockSpec(memory_space=pltpu.VMEM)
    return pl.pallas_call(
        ffn_kernel,
        out_shape=halves(wide),
        in_specs=[pl.BlockSpec(memory_space=pltpu.SMEM), vmem, pl.BlockSpec(memory_space=pltpu.HBM)],
        out_specs=[vmem] * 2,
        scratch_shapes=[
            pltpu.VMEM((wide, WC), BF16),
            pltpu.VMEM((ROWS, GU), F32),
            pltpu.VMEM((ROWS, WC - GU), BF16),
            pltpu.SemaphoreType.DMA((2 * (wide // FC),)),
        ],
        compiler_params=pltpu.CompilerParams(vmem_limit_bytes=48 * 1024 * 1024),
        cost_estimate=pl.CostEstimate(flops=1_700_000_000, bytes_accessed=10_000_000, transcendentals=140_000),
        name="ffn",
    )(core, rows, weights)


def copies(value, axis):
    sent = jnp.broadcast_to(value[None], (lax.axis_size(axis), *value.shape))
    return lax.all_to_all(sent, axis, 0, 0, tiled=True)


def sum_at_owner(mine, theirs):
    given = lax.ppermute(theirs, "c", [(0, 1), (1, 0)])
    both = (mine.astype(F32) + given.astype(F32)).astype(BF16)
    blocks = both.reshape(TPS // 2, OWN, both.shape[1])
    arrived = lax.all_to_all(blocks, "x", 0, 0, tiled=True)
    return arrived.astype(F32).sum(axis=0)


def rms_scale(rows, gain):
    mean_sq = jnp.mean(rows * rows, axis=-1, keepdims=True)
    return rows * lax.rsqrt(mean_sq + EPS) * gain


def shards(
    resid,
    queries,
    keys,
    values,
    log_gates,
    out_gate,
    out_weight,
    post_gain,
    pre_gain,
    ffn_gain,
    gate_weight,
    up_weight,
    down_weight,
):
    pairs = [(row, i, (i + r) % QG, r) for row in ZGRID for i in range(QG) for r in range(1, QG)]
    partner = {a: b for column in zip(*ZGRID) for a, b in (column, column[::-1])}
    asks = [(row[i], row[k], r) for row, i, k, r in pairs if row[i] > min(row[k], partner[row[k]])]

    def ask(r):
        return [(q, k) for q, k, turn in asks if turn == r]

    def answer(r):
        return [(k, q) for q, k, turn in asks if turn == r]

    swap = [(partner[d], d) for row in ZGRID for d in row if max(row) > partner[d]]
    pad = jnp.zeros((gate_weight.shape[0], WC - GU - FFL), BF16)
    packed = jnp.concatenate([gate_weight, up_weight, down_weight.T, pad], axis=1)
    weights = lax.all_gather(packed, SP, axis=0, tiled=True)
    scaled = queries * jnp.asarray(HD**-0.5, BF16)
    q_all = [scaled] + [lax.ppermute(scaled, "z", ask(r)) for r in range(1, QG)]
    held = lax.all_gather(payload(keys.T, values.T, log_gates.T), "y")
    lent = lax.ppermute(held, "z", swap)
    z = lax.axis_index("z")
    zh = sum(jnp.where(z == ZGRID[a][b], a, 0) for a in range(ZH) for b in range(QG))
    zl = sum(jnp.where(z == ZGRID[a][b], b, 0) for a in range(ZH) for b in range(QG))
    pos = jnp.stack([zh, zl, lax.axis_index("y")]).astype(jnp.int32)
    parts = attention(pos, held, lent, *q_all)
    parts = [parts[0]] + [lax.ppermute(parts[r], "z", answer(r)) for r in range(1, QG)]
    core = lax.axis_index("c").astype(jnp.int32)[None]
    projected = sum_at_owner(*merge(core, parts, out_gate, out_weight))
    mixed = resid.astype(F32) + rms_scale(projected, post_gain)
    normed = rms_scale(mixed, pre_gain).astype(BF16)
    along = copies(normed, "x").reshape(ROWS // 2, -1)
    normed_all = lax.all_gather(along, "c", axis=0, tiled=True)
    total = sum_at_owner(*ffn(core, normed_all, weights))
    return (mixed + rms_scale(total, ffn_gain)).astype(BF16)


def solution(mesh):
    split = Mesh(mesh.devices.reshape(8, YS, 4, 2), ("z", "y", "x", "c"))
    in_specs = (
        P((*SP, *TP), None),
        P(SP, TP),
        P(SP, TP),
        P(SP, TP),
        P(SP, TP),
        P(SP, TP),
        P(TP, None),
        P(),
        P(),
        P(),
        P(SP, TP),
        P(SP, TP),
        P(TP, SP),
    )
    return jax.shard_map(
        shards, mesh=split, in_specs=in_specs, out_specs=P((*SP, *TP), None), check_vma=False
    )
```
